512 devices in a mesh: sp: 16 (over y, x), tp: 32 (over z, core).
Axes of the slice: x: 4, y: 4, z: 16, core: 2. Of those that a mesh axis runs over, the one named last changes fastest.
Arguments:
- tokens: bfloat16 [32, 6144, 2048], P('tp', 'sp'), may hold values from -12 to 12
- norm_gain: float32 [2, 2048], replicated, may hold values from 0.1 to 1.9
- in_weight: bfloat16 [2, 2048, 512], P(None, 'sp', 'tp'), may hold values from -0.125 to 0.125
- down_weight: bfloat16 [2, 512, 2048], P(None, 'sp', 'tp'), may hold values from -0.25 to 0.25
- pool_gain: float32 [2, 512], replicated, may hold values from 0.1 to 1.9
Outputs:
- mixed: bfloat16 [32, 6144, 2048], P('tp', 'sp')
The draws below stay inside these ranges and needn't reach their ends.
All inputs are finite; a program needn't handle non-finite values.
Results may differ from the reference program's by a relative error of at most 0.0061.
Values may be sent and summed in bfloat16 or wider, within the bound.
No kernel may reach another device: no remote copies, remote signals or barrier semaphores. Data moves between devices by JAX's collectives and lax.ppermute only.
A program may use at most 64 MiB of HBM per device.

```python
import math
import jax
import jax.numpy as jnp
from jax import lax

D = 2048
P_SIZE = 512
GROUP = 64
LAYERS = 2
TOKENS = 6144
SEQS = 32


def draw_tokens(key, part):
    scale_key, value_key = jax.random.split(jax.random.fold_in(key, 11))
    groups = D // GROUP
    scales = jnp.exp(jax.random.uniform(scale_key, (groups,), jnp.float32, math.log(0.3), math.log(3.0)))
    values = jnp.clip(jax.random.normal(value_key, (SEQS, TOKENS, D), jnp.float32), -4.0, 4.0)
    return (values * jnp.repeat(scales, GROUP)[None, None, :]).astype(jnp.bfloat16)


def levels(rng, extent, shards, low, high):
    def one(dim, blocks):
        draws = jax.random.uniform(jax.random.fold_in(jax.random.fold_in(rng, 6), dim), (blocks,), jnp.float32, low / len(shards), high / len(shards))
        return jnp.repeat(jnp.exp(draws), extent[dim] // blocks).reshape((-1,) + (1,) * (len(extent) - dim - 1))

    level = one(*shards[0])
    for cut in shards[1:]:
        level = level * one(*cut)
    return level


def centred(key, dims, deviation, bound, cuts=(), held_as=jnp.bfloat16):
    drawn = deviation * jax.random.normal(key, dims, jnp.float32)
    if cuts:
        drawn = drawn * levels(key, dims, cuts, -0.22, 0.18)
    return jnp.clip(drawn, -bound, bound).astype(held_as)


def setup_inputs(seed: int = 0) -> dict:
    keys = jax.random.split(jax.random.key(seed), 6)
    tokens = draw_tokens(jax.random.fold_in(keys[5], 71), 0)
    norm_gain = jnp.clip(1.0 + 0.18 * jax.random.normal(keys[1], (LAYERS, D), jnp.float32), 0.1, 1.9)
    in_weight = centred(keys[2], (LAYERS, D, P_SIZE), D ** -0.5, 0.125, ((1, 16), (2, 32)))
    down_weight = centred(keys[3], (LAYERS, P_SIZE, D), P_SIZE ** -0.5, 0.25, ((1, 16), (2, 32)))
    pool_gain = jnp.clip(1.0 + 0.18 * jax.random.normal(keys[4], (LAYERS, P_SIZE), jnp.float32), 0.1, 1.9)
    return {"tokens": tokens, "norm_gain": norm_gain, "in_weight": in_weight, "down_weight": down_weight, "pool_gain": pool_gain}


EPS = 1e-06
WINDOWS = (2, 4, 8, 16)

def pool_rows(extended, first_pos, channel):
    sum_two = extended[1:] + extended[:-1]
    sum_four = sum_two[2:] + sum_two[:-2]
    sum_eight = sum_four[4:] + sum_four[:-4]
    sum_sixteen = sum_eight[8:] + sum_eight[:-8]
    count = extended.shape[0] - 15
    sums = (sum_two[-count:], sum_four[-count:], sum_eight[-count:], sum_sixteen[-count:])
    position = (first_pos + lax.iota(jnp.int32, count) + 1).astype(jnp.float32)
    which_one = channel // GROUP % 4
    result = jnp.zeros((count, extended.shape[1]), jnp.float32)
    for index, window in enumerate(WINDOWS):
        average = sums[index] / jnp.minimum(position, float(window))[:, None]
        result = jnp.where(which_one[None, :] == index, average, result)
    return result - extended[15:]

def reference(tokens, norm_gain, in_weight, down_weight, pool_gain):
    channel = lax.iota(jnp.int32, P_SIZE)

    def one_sequence(stream):
        for layer_index in range(LAYERS):
            residual = stream.astype(jnp.float32)
            inverse_rms = lax.rsqrt(lax.optimization_barrier(jnp.mean(residual * residual, axis=1, keepdims=True)) + EPS)
            normed = (residual * inverse_rms * norm_gain[layer_index]).astype(jnp.bfloat16)
            pool_in = jnp.dot(normed, in_weight[layer_index], preferred_element_type=jnp.float32).astype(jnp.bfloat16)
            extended = jnp.pad(pool_in.astype(jnp.float32), ((15, 0), (0, 0)))
            trailing = pool_rows(extended, jnp.int32(0), channel)
            pooled = (trailing * pool_gain[layer_index]).astype(jnp.bfloat16)
            down = jnp.dot(pooled, down_weight[layer_index], preferred_element_type=jnp.float32)
            stream = (residual + down).astype(jnp.bfloat16)
        return stream
    return lax.map(one_sequence, tokens)
```

```python
import jax
import jax.numpy as jnp
import numpy as np
from jax import lax
from jax.experimental import pallas as pl
from jax.experimental.pallas import tpu as pltpu
from jax.sharding import PartitionSpec as P

GROUP = 64
EPS = 1e-06
WINDOWS = (2, 4, 8, 16)
HALO = 32
NEAR = (1, -1, 2)
SEEN = (0, -1, 1, 2)
AXES = ("sp", "tp")


def number(y, x, z, c):
    return (((y % 4) * 4 + x % 4) * 16 + z % 16) * 2 + c


def send(block, target):
    route = []
    for i in range(512):
        place = (i // 128, i // 32 % 4, i // 2 % 16, i % 2)
        route.append((i, number(*target(*place))))
    return lax.ppermute(block, AXES, route)


def first_hop(d):
    return lambda y, x, z, c: (y, x + d, z, c) if c == 0 else (y + d, x, z, c)


def second_hop(d):
    return lambda y, x, z, c: (y + d, x, z, c) if c == 0 else (y, x + d, z, c)


def other_core(y, x, z, c):
    return y, x, z, 1 - c


def ordered_kernel(place, *refs):
    mine, theirs, whole_in, whole_down = refs[:4], refs[4:8], refs[8], refs[9]
    y, x, c = place[0], place[1], place[2]

    def put_in(pieces):
        for k in range(4):
            row = (y + SEEN[k] + 4) % 4

            def step(i, carry, k=k, row=row):
                r, l = i // 2, i % 2
                seen = jnp.where(r == 0, 0, jnp.where(r == 1, 3, r - 1))
                sp = row * 4 + (x + seen) % 4
                lanes = pl.ds(pl.multiple_of(sp * 128, 128), 128)
                whole_in[l, :, lanes] = pieces[k][r, l]
                return carry

            lax.fori_loop(0, 8, step, 0)

    def put_down(pieces):
        for k in range(4):
            column = (x + SEEN[k] + 4) % 4

            def step(i, carry, k=k, column=column):
                r, l = i // 2, i % 2
                seen = jnp.where(r == 0, 0, jnp.where(r == 1, 3, r - 1))
                sp = (y + seen) % 4 * 4 + column
                rows = pl.ds(pl.multiple_of(sp * 32, 32), 32)
                for j in range(16):
                    whole_down[l, rows, j * 128 : (j + 1) * 128] = pieces[k][
                        r, l, j * 32 : (j + 1) * 32
                    ]
                return carry

            lax.fori_loop(0, 8, step, 0)

    @pl.when(c == 0)
    def _():
        put_in(mine)
        put_down(theirs)

    @pl.when(c == 1)
    def _():
        put_in(theirs)
        put_down(mine)


def ordered(mine, theirs):
    sp, tp = lax.axis_index("sp"), lax.axis_index("tp")
    place = jnp.stack([sp // 4, sp % 4, tp % 2]).astype(jnp.int32)
    whole = jax.ShapeDtypeStruct((2, 512, 2048), jnp.bfloat16)
    vmem = pl.BlockSpec(memory_space=pltpu.VMEM)
    return pl.pallas_call(
        ordered_kernel,
        out_shape=(whole, whole),
        in_specs=[pl.BlockSpec(memory_space=pltpu.SMEM)] + [vmem] * 8,
        out_specs=(vmem, vmem),
        compiler_params=pltpu.CompilerParams(vmem_limit_bytes=24 << 20),
        cost_estimate=pl.CostEstimate(
            flops=4 << 20, bytes_accessed=16 << 20, transcendentals=0
        ),
        name="ordered",
    )(place, *mine, *theirs)


def gathered(in_weight, down_weight):
    core = lax.axis_index("tp") % 2
    layers = in_weight.shape[0]
    turned = jnp.swapaxes(in_weight, 1, 2)
    folded = jnp.concatenate([down_weight[:, :16], down_weight[:, 16:]], axis=2)
    block = jnp.stack([turned, folded])
    column = lax.all_gather(block, "tp")
    col_in = jnp.swapaxes(column[:, 0], 0, 1).reshape(layers, 512, 128)
    col_down = column[:, 1].reshape(16, 2, layers, 16, 2, 64)
    col_down = col_down.transpose(2, 0, 4, 3, 1, 5).reshape(layers, 512, 128)
    own = jnp.where(core == 0, col_in, col_down)
    line = jnp.stack([own] + [send(own, first_hop(d)) for d in NEAR])
    mine = [line] + [send(line, second_hop(d)) for d in NEAR]
    theirs = [send(piece, other_core) for piece in mine]
    return ordered(mine, theirs)


def pool_rows(extended, first_pos, channel):
    sum_two = extended[1:] + extended[:-1]
    sum_four = sum_two[2:] + sum_two[:-2]
    sum_eight = sum_four[4:] + sum_four[:-4]
    sum_sixteen = sum_eight[8:] + sum_eight[:-8]
    count = extended.shape[0] - 15
    sums = (sum_two[-count:], sum_four[-count:], sum_eight[-count:], sum_sixteen)
    position = jnp.maximum(first_pos + lax.iota(jnp.int32, count) + 1, 1)
    position = position.astype(jnp.float32)
    which_one = channel // GROUP % 4
    result = jnp.zeros((count, extended.shape[1]), jnp.float32)
    for index, window in enumerate(WINDOWS):
        average = sums[index] / jnp.minimum(position, float(window))[:, None]
        result = jnp.where(which_one[None, :] == index, average, result)
    return result - extended[15:]


def local(tokens, norm_gain, in_weight, down_weight, pool_gain):
    rows = tokens.shape[1]
    first_pos = lax.axis_index("sp") * rows - HALO
    channel = lax.iota(jnp.int32, pool_gain.shape[1])
    before = lax.ppermute(
        tokens[0, rows - HALO :], AXES, [(i, i + 32) for i in range(480)]
    )
    stream = jnp.concatenate([before, tokens[0]], axis=0)
    whole_in, whole_down = gathered(in_weight, down_weight)
    for l in range(in_weight.shape[0]):
        residual = stream.astype(jnp.float32)
        inverse_rms = lax.rsqrt(
            jnp.mean(residual * residual, axis=1, keepdims=True) + EPS
        )
        normed = (residual * inverse_rms * norm_gain[l]).astype(jnp.bfloat16)
        pool_acc = lax.dot_general(
            normed,
            whole_in[l],
            (((1,), (1,)), ((), ())),
            preferred_element_type=jnp.float32,
        )
        pool_in = pool_acc.astype(jnp.bfloat16).astype(jnp.float32)
        extended = jnp.pad(pool_in, ((15, 0), (0, 0)))
        trailing = pool_rows(extended, first_pos, channel)
        pooled = (trailing * pool_gain[l]).astype(jnp.bfloat16)
        down = jnp.dot(pooled, whole_down[l], preferred_element_type=jnp.float32)
        stream = (residual + down).astype(jnp.bfloat16)
    return stream[HALO:][None]


def solution(mesh):
    in_specs = (P("tp", "sp", None), P(), P(None, "sp", "tp"), P(None, "sp", "tp"), P())
    out_specs = P("tp", "sp", None)
    return jax.shard_map(
        local, mesh=mesh, in_specs=in_specs, out_specs=out_specs, check_vma=False
    )
```

```python
import jax
import jax.numpy as jnp
from jax import lax
from jax.experimental import pallas as pl
from jax.experimental.pallas import tpu as pltpu
from jax.sharding import PartitionSpec as P

EPS = 1e-06
HALO = 32
PAD = 16
SEEN = (0, -1, 1, 2)
AXES = ("sp", "tp")


def number(y, x, z, c):
    return (((y % 4) * 4 + x % 4) * 16 + z % 16) * 2 + c


def places():
    for i in range(512):
        yield i, (i // 128, i // 32 % 4, i // 2 % 16, i % 2)


def send(block, target):
    route = [(i, number(*target(*place))) for i, place in places()]
    return lax.ppermute(block, AXES, route)


def shared(block, count, key):
    groups = {}
    for i, place in places():
        groups.setdefault(key(*place), []).append(i)
    copies = jnp.broadcast_to(block[None], (count, *block.shape))
    return lax.all_to_all(
        copies, AXES, 0, 0, axis_index_groups=list(groups.values()), tiled=True
    )


def second_hop(d):
    return lambda y, x, z, c: (y + d, x, z, c) if c == 0 else (y, x + d, z, c)


def other_core(y, x, z, c):
    return y, x, z, 1 - c


def mixer_kernel(place, halo, tokens, norm_gain, pool_gain, *refs):
    mine, theirs, out = refs[:4], refs[4:8], refs[8]
    whole_in, whole_down, stream, normed, extended, pooled = refs[9:]
    sp, c = place[0], place[1]
    y, x = sp // 4, sp % 4
    s_mine = jnp.where(c == 0, y, x)
    s_theirs = jnp.where(c == 0, x, y)
    left = (lax.broadcasted_iota(jnp.int32, (32, 128), 1) < 64) ^ (c == 1)

    for pieces, core, second in ((mine, c, s_mine), (theirs, 1 - c, s_theirs)):
        for k in range(4):
            s = (second + SEEN[k] + 4) % 4

            def put_in(f, carry, pieces=pieces, core=core, k=k, s=s):
                at = jnp.where(core == 0, s * 4 + f, f * 4 + s)
                lanes = pl.ds(pl.multiple_of(at * 128, 128), 128)
                for l in range(2):
                    whole_in[l, :, core, :, lanes] = pieces[k][
                        f, :, l * 16 : (l + 1) * 16
                    ]
                return carry

            lax.fori_loop(0, 4, put_in, 0)

    for k in range(4):
        a = (s_mine + SEEN[k] + 4) % 4
        for j in range(4):
            b = (s_theirs + SEEN[j] + 4) % 4
            at = jnp.where(c == 0, a * 4 + b, b * 4 + a)
            rows = pl.ds(pl.multiple_of(at * 32, 32), 32)
            for z in range(16):
                m = mine[k][b, z, 32:64]
                t = theirs[j][a, z, 32:64]
                lanes = slice(z * 128, (z + 1) * 128)
                whole_down[0, rows, lanes] = jnp.where(left, m, t)
                v = jnp.where(left, t, m)
                whole_down[1, rows, lanes] = jnp.concatenate(
                    [v[:, 64:], v[:, :64]], axis=1
                )

    stream[:HALO] = halo[...]
    stream[HALO:] = tokens[...]
    extended[:PAD] = jnp.zeros((PAD, 512), jnp.float32)
    count = extended.shape[0] - PAD
    row = lax.broadcasted_iota(jnp.int32, (count, 128), 0)
    lane = lax.broadcasted_iota(jnp.int32, (count, 128), 1)
    position = jnp.maximum(sp * 384 - HALO + row + 1, 1).astype(jnp.float32)

    def layer(l, carry):
        gain_in = jnp.where(l == 0, norm_gain[0:1], norm_gain[1:2])

        def norm(i, carry):
            rows = pl.ds(pl.multiple_of(i * 32, 32), 32)
            residual = stream[rows].astype(jnp.float32)
            mean = jnp.mean(residual * residual, axis=1, keepdims=True)
            scaled = residual * lax.rsqrt(mean + EPS) * gain_in
            normed[rows] = scaled.astype(jnp.bfloat16)
            return carry

        lax.fori_loop(0, count // 32, norm, 0)
        pool_in = lax.dot_general(
            normed[...],
            whole_in[l].reshape(512, 2048),
            (((1,), (1,)), ((), ())),
            preferred_element_type=jnp.float32,
        )
        extended[PAD:] = pool_in.astype(jnp.bfloat16).astype(jnp.float32)
        for j in range(4):
            lanes = slice(j * 128, (j + 1) * 128)
            own = extended[:, lanes]
            two = own + pltpu.roll(own, 1, 0)
            four = two + pltpu.roll(two, 2, 0)
            short, long, window = two, four, 2.0
            if j % 2:
                eight = four + pltpu.roll(four, 4, 0)
                short, long, window = eight, eight + pltpu.roll(eight, 8, 0), 8.0
            total = jnp.where(lane < 64, short[PAD:], long[PAD:])
            width = jnp.where(lane < 64, window, 2 * window)
            trailing = total / jnp.minimum(position, width) - own[PAD:]
            gain = jnp.where(l == 0, pool_gain[0:1, lanes], pool_gain[1:2, lanes])
            pooled[:, lanes] = (trailing * gain).astype(jnp.bfloat16)
        for j in range(4):
            lanes = slice(j * 512, (j + 1) * 512)
            down = jnp.dot(
                pooled[...],
                whole_down[l, :, lanes],
                preferred_element_type=jnp.float32,
            )
            total = stream[:, lanes].astype(jnp.float32) + down
            stream[:, lanes] = total.astype(jnp.bfloat16)
        return carry

    lax.fori_loop(0, 2, layer, 0)
    out[...] = stream[HALO:]


def mixer(halo, tokens, norm_gain, pool_gain, mine, theirs):
    place = jnp.stack([lax.axis_index("sp"), lax.axis_index("tp") % 2])
    vmem = pl.BlockSpec(memory_space=pltpu.VMEM)
    rows = HALO + tokens.shape[0]
    return pl.pallas_call(
        mixer_kernel,
        out_shape=jax.ShapeDtypeStruct(tokens.shape, tokens.dtype),
        in_specs=[pl.BlockSpec(memory_space=pltpu.SMEM)] + [vmem] * 12,
        out_specs=vmem,
        scratch_shapes=[
            pltpu.VMEM((2, 16, 2, 16, 2048), jnp.bfloat16),
            pltpu.VMEM((2, 512, 2048), jnp.bfloat16),
            pltpu.VMEM((rows, 2048), jnp.bfloat16),
            pltpu.VMEM((rows, 2048), jnp.bfloat16),
            pltpu.VMEM((PAD + rows, 512), jnp.float32),
            pltpu.VMEM((rows, 512), jnp.bfloat16),
        ],
        compiler_params=pltpu.CompilerParams(vmem_limit_bytes=26 << 20),
        cost_estimate=pl.CostEstimate(
            flops=4 << 30, bytes_accessed=16 << 20, transcendentals=0
        ),
        name="mixer",
    )(place.astype(jnp.int32), halo, tokens, norm_gain, pool_gain, *mine, *theirs)


def gathered(in_weight, down_weight):
    core = lax.axis_index("tp") % 2
    turned = jnp.swapaxes(in_weight, 1, 2).reshape(32, 128)
    first = jnp.where(core == 0, down_weight[0], down_weight[1])
    last = jnp.where(core == 0, down_weight[1], down_weight[0])
    folded = jnp.concatenate([first, last], axis=1)
    block = jnp.concatenate([turned, folded], axis=0)
    column = shared(block, 16, lambda y, x, z, c: (y, x, c))
    line = shared(
        column.reshape(16, 64, 128),
        4,
        lambda y, x, z, c: (y, z, c) if c == 0 else (x, z, c),
    )
    line = line.reshape(4, 16, 64, 128)
    mine = [line]
    for d in (1, -1, 2):
        mine.append(send(line, second_hop(d)))
    theirs = []
    for piece in mine:
        theirs.append(send(piece, other_core))
    return mine, theirs


def mixed(tokens, norm_gain, in_weight, down_weight, pool_gain):
    rows = tokens.shape[1]
    halo = lax.ppermute(
        tokens[0, rows - HALO :], AXES, [(i, i + 32) for i in range(480)]
    )
    mine, theirs = gathered(in_weight, down_weight)
    return mixer(halo, tokens[0], norm_gain, pool_gain, mine, theirs)[None]


def solution(mesh):
    in_specs = (P("tp", "sp", None), P(), P(None, "sp", "tp"), P(None, "sp", "tp"), P())
    out_specs = P("tp", "sp", None)
    return jax.shard_map(
        mixed, mesh=mesh, in_specs=in_specs, out_specs=out_specs, check_vma=False
    )
```

```python
import jax
import jax.numpy as jnp
from jax import lax
from jax.experimental import pallas as pl
from jax.experimental.pallas import tpu as pltpu
from jax.sharding import PartitionSpec as P

EPS = 1e-06
HALO = 32
PAD = 16
AXES = ("sp", "tp")
PIECES = ((0, 0, 4), (-1, 0, 4), (1, 0, 4), (2, 0, 2), (2, 2, 4))
HEAD_MIB, PUT_MIB, MIX_MIB = 5, 10, 16
VMEM = pl.BlockSpec(memory_space=pltpu.VMEM)
SMEM = pl.BlockSpec(memory_space=pltpu.SMEM)


def number(y, x, z, c):
    return (((y % 4) * 4 + x % 4) * 16 + z % 16) * 2 + c


def places():
    for i in range(512):
        yield i, (i // 128, i // 32 % 4, i // 2 % 16, i % 2)


def send(block, target):
    route = [(i, number(*target(*place))) for i, place in places()]
    return lax.ppermute(block, AXES, route)


def shared(block, count, key):
    groups = {}
    for i, place in places():
        groups.setdefault(key(*place), []).append(i)
    copies = jnp.broadcast_to(block[None], (count, *block.shape))
    return lax.all_to_all(
        copies, AXES, 0, 0, axis_index_groups=list(groups.values()), tiled=True
    )


def second_hop(d):
    return lambda y, x, z, c: (y + d, x, z, c) if c == 0 else (y, x + d, z, c)


def other_core(y, x, z, c):
    return y, x, z, 1 - c


def seconds(place):
    sp, c = place[0], place[1]
    y, x = sp // 4, sp % 4
    return c, jnp.where(c == 0, y, x), jnp.where(c == 0, x, y)


def put(place, mine, theirs, new, whole_in, whole_down):
    c, s_mine, s_theirs = seconds(place)
    left = (lax.broadcasted_iota(jnp.int32, (32, 128), 1) < 64) ^ (c == 1)

    for pieces, core, second in ((mine, c, s_mine), (theirs, 1 - c, s_theirs)):
        for k in new:
            d, low, high = PIECES[k]
            s = (second + d + 4) % 4

            def put_in(i, carry, pieces=pieces, core=core, k=k, s=s, low=low):
                f = i + low
                at = jnp.where(core == 0, s * 4 + f, f * 4 + s)
                lanes = pl.ds(pl.multiple_of(at * 128, 128), 128)
                for l in range(2):
                    whole_in[l, :, core, :, lanes] = pieces[k][
                        i, :, l * 16 : (l + 1) * 16
                    ]
                return carry

            lax.fori_loop(0, high - low, put_in, 0)

    for k in range(max(new) + 1):
        for j in range(max(new) + 1):
            if k not in new and j not in new:
                continue
            a = (s_mine + PIECES[k][0] + 4) % 4
            b = (s_theirs + PIECES[j][0] + 4) % 4
            (_, k_low, k_high), (_, j_low, j_high) = PIECES[k], PIECES[j]

            def put_down(k=k, j=j, a=a, b=b, k_low=k_low, j_low=j_low):
                at = jnp.where(c == 0, a * 4 + b, b * 4 + a)
                rows = pl.ds(pl.multiple_of(at * 32, 32), 32)
                for z in range(16):
                    m = mine[k][b - k_low, z, 32:64]
                    t = theirs[j][a - j_low, z, 32:64]
                    lanes = slice(z * 128, (z + 1) * 128)
                    whole_down[0, rows, lanes] = jnp.where(left, m, t)
                    v = jnp.where(left, t, m)
                    whole_down[1, rows, lanes] = jnp.concatenate(
                        [v[:, 64:], v[:, :64]], axis=1
                    )

            if k > 2 or j > 2:
                here = (b >= k_low) & (b < k_high) & (a >= j_low) & (a < j_high)
                pl.when(here)(put_down)
            else:
                put_down()


def wholes():
    return (
        jax.ShapeDtypeStruct((2, 16, 2, 16, 2048), jnp.bfloat16),
        jax.ShapeDtypeStruct((2, 512, 2048), jnp.bfloat16),
    )


def params(mib):
    return pltpu.CompilerParams(vmem_limit_bytes=mib << 20)


def cost(flops):
    return pl.CostEstimate(flops=flops, bytes_accessed=1 << 20, transcendentals=0)


def placed(place, mine, theirs, new, wholes_before=()):
    count = max(new) + 1

    def kernel(place, *refs):
        put(place, refs[:count], refs[count : 2 * count], new, refs[-2], refs[-1])

    at = 1 + 2 * count
    return pl.pallas_call(
        kernel,
        out_shape=wholes(),
        in_specs=[SMEM] + [VMEM] * (2 * count + len(wholes_before)),
        out_specs=(VMEM, VMEM),
        input_output_aliases={at: 0, at + 1: 1} if wholes_before else {},
        compiler_params=params(PUT_MIB),
        cost_estimate=cost(1 << 29),
    )(place, *mine[:count], *theirs[:count], *wholes_before)


def norm_rows(block, gain):
    residual = block.astype(jnp.float32)
    mean = jnp.mean(residual * residual, axis=1, keepdims=True)
    return (residual * lax.rsqrt(mean + EPS) * gain).astype(jnp.bfloat16)


def head_kernel(tokens, norm_gain, normed):
    def norm(i, carry):
        rows = pl.multiple_of(i * 32, 32)
        normed[pl.ds(HALO + rows, 32)] = norm_rows(
            tokens[pl.ds(rows, 32)], norm_gain[0:1]
        )
        return carry

    lax.fori_loop(0, tokens.shape[0] // 32, norm, 0)


def head(tokens, norm_gain):
    return pl.pallas_call(
        head_kernel,
        out_shape=jax.ShapeDtypeStruct((HALO + tokens.shape[0], 2048), jnp.bfloat16),
        in_specs=[VMEM] * 2,
        out_specs=VMEM,
        compiler_params=params(HEAD_MIB),
        cost_estimate=cost(1 << 30),
        name="head",
    )(tokens, norm_gain)


def mixer_kernel(place, halo, tokens, normed, norm_gain, pool_gain, *refs):
    count = len(PIECES)
    mine, theirs = refs[:count], refs[count : 2 * count]
    out, whole_in, whole_down, left, extended, pooled, middle = refs[-7:]
    put(place, mine, theirs, (3, 4), whole_in, whole_down)
    rows = left.shape[0]
    left[:HALO] = norm_rows(halo[...], norm_gain[0:1])
    extended[:PAD] = jnp.zeros((PAD, 512), jnp.float32)
    row = lax.broadcasted_iota(jnp.int32, (rows, 128), 0)
    lane = lax.broadcasted_iota(jnp.int32, (rows, 128), 1)
    position = place[0] * 384 - HALO + row + 1
    position = jnp.maximum(position, 1).astype(jnp.float32)

    def pool(l, row_scale):
        pool_in = lax.dot_general(
            left[...],
            whole_in[l].reshape(512, 2048),
            (((1,), (1,)), ((), ())),
            preferred_element_type=jnp.float32,
        )
        if row_scale is not None:
            pool_in = pool_in * row_scale
        extended[PAD:] = pool_in.astype(jnp.bfloat16).astype(jnp.float32)
        for j in range(4):
            lanes = slice(j * 128, (j + 1) * 128)
            own = extended[:, lanes]
            two = own + pltpu.roll(own, 1, 0)
            four = two + pltpu.roll(two, 2, 0)
            short, long, window = two, four, 2.0
            if j % 2:
                eight = four + pltpu.roll(four, 4, 0)
                short, long, window = eight, eight + pltpu.roll(eight, 8, 0), 8.0
            total = jnp.where(lane < 64, short[PAD:], long[PAD:])
            width = jnp.where(lane < 64, window, 2 * window)
            trailing = total / jnp.minimum(position, width) - own[PAD:]
            gain = pool_gain[l : l + 1, lanes]
            pooled[:, lanes] = (trailing * gain).astype(jnp.bfloat16)

    pool(0, None)
    squares = jnp.zeros((rows, 128), jnp.float32)
    for j in range(4):
        lanes = slice(j * 512, (j + 1) * 512)
        down = jnp.dot(
            pooled[...], whole_down[0, :, lanes], preferred_element_type=jnp.float32
        )
        before = jnp.concatenate([halo[:, lanes], tokens[:, lanes]], axis=0)
        total = before.astype(jnp.float32) + down
        middle[:, lanes] = total.astype(jnp.bfloat16)
        total = middle[:, lanes].astype(jnp.float32)
        left[:, lanes] = (total * norm_gain[1:2, lanes]).astype(jnp.bfloat16)
        total = total * total
        squares += (total[:, :128] + total[:, 128:256]) + (
            total[:, 256:384] + total[:, 384:]
        )
    mean = jnp.sum(squares, axis=1, keepdims=True) / 2048.0
    pool(1, lax.rsqrt(mean + EPS))
    for j in range(4):
        lanes = slice(j * 512, (j + 1) * 512)
        down = jnp.dot(
            pooled[HALO:], whole_down[1, :, lanes], preferred_element_type=jnp.float32
        )
        total = middle[HALO:, lanes].astype(jnp.float32) + down
        out[:, lanes] = total.astype(jnp.bfloat16)


def mixer(place, halo, tokens, normed, norm_gain, pool_gain, mine, theirs, whole):
    rows = normed.shape[0]
    at = 6 + 2 * len(PIECES)
    return pl.pallas_call(
        mixer_kernel,
        out_shape=(
            jax.ShapeDtypeStruct(tokens.shape, tokens.dtype),
            *wholes(),
            jax.ShapeDtypeStruct(normed.shape, normed.dtype),
        ),
        in_specs=[SMEM] + [VMEM] * (at + 1),
        out_specs=(VMEM,) * 4,
        input_output_aliases={at: 1, at + 1: 2, 3: 3},
        scratch_shapes=[
            pltpu.VMEM((PAD + rows, 512), jnp.float32),
            pltpu.VMEM((rows, 512), jnp.bfloat16),
            pltpu.VMEM((rows, 2048), jnp.bfloat16),
        ],
        compiler_params=params(MIX_MIB),
        cost_estimate=cost(4 << 30),
        name="mixer",
    )(place, halo, tokens, normed, norm_gain, pool_gain, *mine, *theirs, *whole)[0]


def packed(in_weight, down_weight):
    core = lax.axis_index("tp") % 2
    turned = jnp.swapaxes(in_weight, 1, 2).reshape(32, 128)
    first = jnp.where(core == 0, down_weight[0], down_weight[1])
    last = jnp.where(core == 0, down_weight[1], down_weight[0])
    return jnp.concatenate([turned, jnp.concatenate([first, last], axis=1)], axis=0)


def mixed(tokens, norm_gain, in_weight, down_weight, pool_gain):
    rows = tokens.shape[1]
    place = jnp.stack([lax.axis_index("sp"), lax.axis_index("tp") % 2])
    place = place.astype(jnp.int32)
    halo = lax.ppermute(
        tokens[0, rows - HALO :], AXES, [(i, i + 32) for i in range(480)]
    )
    normed = head(tokens[0], norm_gain)
    column = shared(packed(in_weight, down_weight), 16, lambda y, x, z, c: (y, x, c))
    line = shared(
        column.reshape(16, 64, 128),
        4,
        lambda y, x, z, c: (y, z, c) if c == 0 else (x, z, c),
    )
    line = line.reshape(4, 16, 64, 128)
    up = send(line, second_hop(1))
    down = send(line, second_hop(-1))
    up_on = send(up[:2], second_hop(1))
    down_on = send(down[2:], second_hop(-1))
    mine = [line, up, down, up_on, down_on]
    theirs = [send(piece, other_core) for piece in mine]
    whole = placed(place, mine, theirs, (0,))
    whole = placed(place, mine, theirs, (1, 2), whole)
    return mixer(
        place, halo, tokens[0], normed, norm_gain, pool_gain, mine, theirs, whole
    )[None]


def solution(mesh):
    in_specs = (P("tp", "sp", None), P(), P(None, "sp", "tp"), P(None, "sp", "tp"), P())
    out_specs = P("tp", "sp", None)
    return jax.shard_map(
        mixed, mesh=mesh, in_specs=in_specs, out_specs=out_specs, check_vma=False
    )
```

```python
import jax
import jax.numpy as jnp
from jax import lax
from jax.experimental import pallas as pl
from jax.experimental.pallas import tpu as pltpu
from jax.sharding import PartitionSpec as P

EPS = 1e-06
HALO = 32
PAD = 16
AXES = ("sp", "tp")
PIECES = (0, 2, 1, -1)
HEAD_MIB, PUT_MIB, MIX_MIB = 5, 10, 16
VMEM = pl.BlockSpec(memory_space=pltpu.VMEM)
SMEM = pl.BlockSpec(memory_space=pltpu.SMEM)


def number(y, x, z, c):
    return (((y % 4) * 4 + x % 4) * 16 + z % 16) * 2 + c


def places():
    for i in range(512):
        yield i, (i // 128, i // 32 % 4, i // 2 % 16, i % 2)


def send(block, target):
    route = [(i, number(*target(*place))) for i, place in places()]
    return lax.ppermute(block, AXES, route)


def shared(block, count, key):
    groups = {}
    for i, place in places():
        groups.setdefault(key(*place), []).append(i)
    copies = jnp.broadcast_to(block[None], (count, *block.shape))
    return lax.all_to_all(
        copies, AXES, 0, 0, axis_index_groups=list(groups.values()), tiled=True
    )


def second_hop(d):
    return lambda y, x, z, c: (y + d, x, z, c) if c == 0 else (y, x + d, z, c)


def other_core(y, x, z, c):
    return y, x, z, 1 - c


def seconds(place):
    sp, c = place[0], place[1]
    y, x = sp // 4, sp % 4
    return c, jnp.where(c == 0, y, x), jnp.where(c == 0, x, y)


def put(place, mine, theirs, new, whole_in, whole_down):
    c, s_mine, s_theirs = seconds(place)
    left = (lax.broadcasted_iota(jnp.int32, (32, 128), 1) < 64) ^ (c == 1)

    for pieces, core, second in ((mine, c, s_mine), (theirs, 1 - c, s_theirs)):
        for k in new:
            s = (second + PIECES[k] + 4) % 4

            def put_in(f, carry, pieces=pieces, core=core, k=k, s=s):
                at = jnp.where(core == 0, s * 4 + f, f * 4 + s)
                lanes = pl.ds(pl.multiple_of(at * 128, 128), 128)
                for l in range(2):
                    whole_in[l, :, core, :, lanes] = pieces[k][
                        f, :, l * 16 : (l + 1) * 16
                    ]
                return carry

            lax.fori_loop(0, 4, put_in, 0)

    for k in range(max(new) + 1):
        for j in range(max(new) + 1):
            if k not in new and j not in new:
                continue
            a = (s_mine + PIECES[k] + 4) % 4
            b = (s_theirs + PIECES[j] + 4) % 4
            at = jnp.where(c == 0, a * 4 + b, b * 4 + a)
            rows = pl.ds(pl.multiple_of(at * 32, 32), 32)
            for z in range(16):
                m = mine[k][b, z, 32:64]
                t = theirs[j][a, z, 32:64]
                lanes = slice(z * 128, (z + 1) * 128)
                whole_down[0, rows, lanes] = jnp.where(left, m, t)
                v = jnp.where(left, t, m)
                whole_down[1, rows, lanes] = jnp.concatenate(
                    [v[:, 64:], v[:, :64]], axis=1
                )


def wholes():
    return (
        jax.ShapeDtypeStruct((2, 16, 2, 16, 2048), jnp.bfloat16),
        jax.ShapeDtypeStruct((2, 512, 2048), jnp.bfloat16),
    )


def params(mib):
    return pltpu.CompilerParams(vmem_limit_bytes=mib << 20)


def cost(flops):
    return pl.CostEstimate(flops=flops, bytes_accessed=1 << 20, transcendentals=0)


def placed(place, mine, theirs, new, wholes_before=()):
    count = max(new) + 1

    def kernel(place, *refs):
        put(place, refs[:count], refs[count : 2 * count], new, refs[-2], refs[-1])

    at = 1 + 2 * count
    return pl.pallas_call(
        kernel,
        out_shape=wholes(),
        in_specs=[SMEM] + [VMEM] * (2 * count + len(wholes_before)),
        out_specs=(VMEM, VMEM),
        input_output_aliases={at: 0, at + 1: 1} if wholes_before else {},
        compiler_params=params(PUT_MIB),
        cost_estimate=cost(1 << 29),
    )(place, *mine[:count], *theirs[:count], *wholes_before)


def norm_rows(block, gain):
    residual = block.astype(jnp.float32)
    mean = jnp.mean(residual * residual, axis=1, keepdims=True)
    return (residual * lax.rsqrt(mean + EPS) * gain).astype(jnp.bfloat16)


def head_kernel(tokens, norm_gain, normed):
    def norm(i, carry):
        rows = pl.multiple_of(i * 32, 32)
        normed[pl.ds(HALO + rows, 32)] = norm_rows(
            tokens[pl.ds(rows, 32)], norm_gain[0:1]
        )
        return carry

    lax.fori_loop(0, tokens.shape[0] // 32, norm, 0)


def head(tokens, norm_gain):
    return pl.pallas_call(
        head_kernel,
        out_shape=jax.ShapeDtypeStruct((HALO + tokens.shape[0], 2048), jnp.bfloat16),
        in_specs=[VMEM] * 2,
        out_specs=VMEM,
        compiler_params=params(HEAD_MIB),
        cost_estimate=cost(1 << 30),
        name="head",
    )(tokens, norm_gain)


def mixer_kernel(place, halo, tokens, normed, norm_gain, pool_gain, *refs):
    count = len(PIECES)
    mine, theirs = refs[:count], refs[count : 2 * count]
    out, whole_in, whole_down, left, extended, pooled, middle, last, sems = refs[-9:]
    put(place, mine, theirs, (2, 3), whole_in, whole_down)
    rows = left.shape[0]
    left[:HALO] = norm_rows(halo[...], norm_gain[0:1])
    extended[:PAD] = jnp.zeros((PAD, 512), jnp.float32)
    row = lax.broadcasted_iota(jnp.int32, (rows, 128), 0)
    lane = lax.broadcasted_iota(jnp.int32, (rows, 128), 1)
    position = place[0] * 384 - HALO + row + 1
    position = jnp.maximum(position, 1).astype(jnp.float32)

    def pool(l, row_scale):
        pool_in = lax.dot_general(
            left[...],
            whole_in[l].reshape(512, 2048),
            (((1,), (1,)), ((), ())),
            preferred_element_type=jnp.float32,
        )
        if row_scale is not None:
            pool_in = pool_in * row_scale
        extended[PAD:] = pool_in.astype(jnp.bfloat16).astype(jnp.float32)
        for j in range(4):
            lanes = slice(j * 128, (j + 1) * 128)
            own = extended[:, lanes]
            two = own + pltpu.roll(own, 1, 0)
            four = two + pltpu.roll(two, 2, 0)
            short, long, window = two, four, 2.0
            if j % 2:
                eight = four + pltpu.roll(four, 4, 0)
                short, long, window = eight, eight + pltpu.roll(eight, 8, 0), 8.0
            total = jnp.where(lane < 64, short[PAD:], long[PAD:])
            width = jnp.where(lane < 64, window, 2 * window)
            trailing = total / jnp.minimum(position, width) - own[PAD:]
            gain = pool_gain[l : l + 1, lanes]
            pooled[:, lanes] = (trailing * gain).astype(jnp.bfloat16)

    pool(0, None)
    squares = jnp.zeros((rows, 128), jnp.float32)
    for j in range(4):
        lanes = slice(j * 512, (j + 1) * 512)
        down = jnp.dot(
            pooled[...], whole_down[0, :, lanes], preferred_element_type=jnp.float32
        )
        before = jnp.concatenate([halo[:, lanes], tokens[:, lanes]], axis=0)
        total = before.astype(jnp.float32) + down
        middle[:, lanes] = total.astype(jnp.bfloat16)
        total = middle[:, lanes].astype(jnp.float32)
        left[:, lanes] = (total * norm_gain[1:2, lanes]).astype(jnp.bfloat16)
        total = total * total
        squares += (total[:, :128] + total[:, 128:256]) + (
            total[:, 256:384] + total[:, 384:]
        )
    mean = jnp.sum(squares, axis=1, keepdims=True) / 2048.0
    pool(1, lax.rsqrt(mean + EPS))
    copies = []
    for j in range(4):
        lanes = slice(j * 512, (j + 1) * 512)
        down = jnp.dot(
            pooled[HALO:], whole_down[1, :, lanes], preferred_element_type=jnp.float32
        )
        total = middle[HALO:, lanes].astype(jnp.float32) + down
        last[:, lanes] = total.astype(jnp.bfloat16)
        copies.append(pltpu.make_async_copy(last.at[:, lanes], out.at[:, lanes], sems.at[j]))
        copies[-1].start()
    for copy in copies:
        copy.wait()


def mixer(place, halo, tokens, normed, norm_gain, pool_gain, mine, theirs, whole):
    rows = normed.shape[0]
    at = 6 + 2 * len(PIECES)
    return pl.pallas_call(
        mixer_kernel,
        out_shape=(
            jax.ShapeDtypeStruct(tokens.shape, tokens.dtype),
            *wholes(),
            jax.ShapeDtypeStruct(normed.shape, normed.dtype),
        ),
        in_specs=[SMEM] + [VMEM] * (at + 1),
        out_specs=(pl.BlockSpec(memory_space=pl.ANY),) + (VMEM,) * 3,
        input_output_aliases={at: 1, at + 1: 2, 3: 3},
        scratch_shapes=[
            pltpu.VMEM((PAD + rows, 512), jnp.float32),
            pltpu.VMEM((rows, 512), jnp.bfloat16),
            pltpu.VMEM((rows, 2048), jnp.bfloat16),
            pltpu.VMEM(tokens.shape, jnp.bfloat16),
            pltpu.SemaphoreType.DMA((4,)),
        ],
        compiler_params=params(MIX_MIB),
        cost_estimate=cost(4 << 30),
        name="mixer",
    )(place, halo, tokens, normed, norm_gain, pool_gain, *mine, *theirs, *whole)[0]


def packed(in_weight, down_weight):
    core = lax.axis_index("tp") % 2
    turned = jnp.swapaxes(in_weight, 1, 2).reshape(32, 128)
    first = jnp.where(core == 0, down_weight[0], down_weight[1])
    last = jnp.where(core == 0, down_weight[1], down_weight[0])
    return jnp.concatenate([turned, jnp.concatenate([first, last], axis=1)], axis=0)


def mixed(tokens, norm_gain, in_weight, down_weight, pool_gain):
    rows = tokens.shape[1]
    place = jnp.stack([lax.axis_index("sp"), lax.axis_index("tp") % 2])
    place = place.astype(jnp.int32)
    halo = lax.ppermute(
        tokens[0, rows - HALO :], AXES, [(i, i + 32) for i in range(480)]
    )
    normed = head(tokens[0], norm_gain)
    column = shared(packed(in_weight, down_weight), 16, lambda y, x, z, c: (y, x, c))
    line = shared(
        column.reshape(16, 64, 128),
        4,
        lambda y, x, z, c: (y, z, c) if c == 0 else (x, z, c),
    )
    line = line.reshape(4, 16, 64, 128)
    names = (2, -1, 1)
    mine = [line] + [send(line, second_hop(d)) for d in names]
    theirs = [send(piece, other_core) for piece in mine]
    whole = placed(place, mine, theirs, (0,))
    whole = placed(place, mine, theirs, (1,), whole)
    return mixer(
        place, halo, tokens[0], normed, norm_gain, pool_gain, mine, theirs, whole
    )[None]


def solution(mesh):
    in_specs = (P("tp", "sp", None), P(), P(None, "sp", "tp"), P(None, "sp", "tp"), P())
    out_specs = P("tp", "sp", None)
    return jax.shard_map(
        mixed, mesh=mesh, in_specs=in_specs, out_specs=out_specs, check_vma=False
    )
```

```python
import jax
import jax.numpy as jnp
from jax import lax
from jax.experimental import pallas as pl
from jax.experimental.pallas import tpu as pltpu
from jax.sharding import PartitionSpec as P

EPS = 1e-06
HALO = 32
PAD = 16
AXES = ("sp", "tp")
PIECES = (0, 2, 1, -1)
VMEM = pl.BlockSpec(memory_space=pltpu.VMEM)
BF16, F32 = jnp.bfloat16, jnp.float32


def number(y, x, z, c):
    return (((y % 4) * 4 + x % 4) * 16 + z % 16) * 2 + c


def places():
    for i in range(512):
        yield i, (i // 128, i // 32 % 4, i // 2 % 16, i % 2)


def send(block, target):
    route = [(i, number(*target(*place))) for i, place in places()]
    return lax.ppermute(block, AXES, route)


def shared(copies, key):
    groups = {}
    for i, place in places():
        groups.setdefault(key(*place), []).append(i)
    return lax.all_to_all(
        copies, AXES, 0, 0, axis_index_groups=list(groups.values()), tiled=True
    )


def second_hop(d):
    return lambda y, x, z, c: (y + d, x, z, c) if c == 0 else (y, x + d, z, c)


def other_core(y, x, z, c):
    return y, x, z, 1 - c


def seconds():
    sp, c = lax.axis_index("sp"), lax.axis_index("tp") % 2
    y, x = sp // 4, sp % 4
    return c, jnp.where(c == 0, y, x), jnp.where(c == 0, x, y)


def lanes_of(core, s, f):
    at = jnp.where(core == 0, s * 4 + f, f * 4 + s)
    return pl.ds(pl.multiple_of(at * 128, 128), 128)


def along(second, k):
    return (second + PIECES[k] + 4) % 4


def part(left, piece, core, s):
    lhs = jnp.concatenate([left[:, lanes_of(core, s, f)] for f in range(4)], axis=1)
    rhs = jnp.concatenate(
        [piece[f, :, 0:16].reshape(256, 128) for f in range(4)], axis=1
    )
    return lax.dot_general(
        lhs, rhs, (((1,), (1,)), ((), ())), preferred_element_type=F32
    )


def put_in(piece, core, s, whole_in):
    def step(f, carry):
        whole_in[core, :, :, lanes_of(core, s, f)] = piece[f, :, 16:32]
        return carry

    lax.fori_loop(0, 4, step, 0)


def put_down(mine, theirs, pairs, whole_down):
    c, s_mine, s_theirs = seconds()
    left = (lax.broadcasted_iota(jnp.int32, (32, 128), 1) < 64) ^ (c == 1)
    for k, j in pairs:
        a, b = along(s_mine, k), along(s_theirs, j)
        at = jnp.where(c == 0, a * 4 + b, b * 4 + a)
        rows = pl.ds(pl.multiple_of(at * 16, 16), 16)
        for z in range(16):
            m = mine[k][b, z, 32:64]
            t = theirs[j][a, z, 32:64]
            lanes = slice(z * 128, (z + 1) * 128)
            first = jnp.where(left, m, t)
            last = jnp.where(left, t, m)
            last = jnp.concatenate([last[:, 64:], last[:, :64]], axis=1)
            for l, tile in enumerate((first, last)):
                whole_down[l, 0, rows, lanes] = tile[:16]
                whole_down[l, 1, rows, lanes] = tile[16:]


def params(mib):
    return pltpu.CompilerParams(vmem_limit_bytes=mib << 20)


def cost(flops):
    return pl.CostEstimate(flops=flops, bytes_accessed=1 << 20, transcendentals=0)


def packed(in_weight, down_weight):
    core = lax.axis_index("tp") % 2
    turned = jnp.swapaxes(in_weight, 1, 2).reshape(32, 128)
    first = jnp.where(core == 0, down_weight[0], down_weight[1])
    last = jnp.where(core == 0, down_weight[1], down_weight[0])
    folded = jnp.concatenate([first, last], axis=1)
    block = jnp.concatenate([turned, folded], axis=0)
    return jnp.broadcast_to(block[None], (16, 64, 128))


def head_kernel(halo, tokens, norm_gain, pool_gain, normed, gain_out):
    gain = norm_gain[0:1]

    def norm_rows(block):
        residual = block.astype(F32)
        mean = jnp.mean(residual * residual, axis=1, keepdims=True)
        return (residual * lax.rsqrt(mean + EPS) * gain).astype(BF16)

    def norm(i, carry):
        rows = pl.multiple_of(i * 32, 32)
        normed[pl.ds(HALO + rows, 32)] = norm_rows(tokens[pl.ds(rows, 32)])
        return carry

    lax.fori_loop(0, tokens.shape[0] // 32, norm, 0)
    normed[:HALO] = norm_rows(halo[...])
    old = lax.broadcasted_iota(jnp.int32, (512, 512), 0)
    new = lax.broadcasted_iota(jnp.int32, (512, 512), 1)
    source = new % 256 // 16 * 32 + new // 256 * 16 + new % 16
    gain_out[...] = jnp.dot(
        pool_gain[...],
        (old == source).astype(F32),
        precision=lax.Precision.HIGHEST,
        preferred_element_type=F32,
    )


def head(halo, tokens, norm_gain, pool_gain):
    return pl.pallas_call(
        head_kernel,
        out_shape=(
            jax.ShapeDtypeStruct((HALO + tokens.shape[0], 2048), BF16),
            jax.ShapeDtypeStruct(pool_gain.shape, F32),
        ),
        in_specs=[VMEM] * 4,
        out_specs=(VMEM, VMEM),
        compiler_params=params(5),
        cost_estimate=cost(1 << 30),
        name="head",
    )(halo, tokens, norm_gain, pool_gain)


def wholes():
    return (
        jax.ShapeDtypeStruct((2, 16, 16, 2048), BF16),
        jax.ShapeDtypeStruct((2, 2, 256, 2048), BF16),
    )


def placed(body, mib, normed, pieces, so_far):
    rows = normed.shape[0]
    count = 1 + len(pieces)

    def kernel(*refs):
        body(refs[0], refs[1:count], refs[count:-3], *refs[-3:])

    return pl.pallas_call(
        kernel,
        out_shape=(jax.ShapeDtypeStruct((2, rows, 256), F32), *wholes()),
        in_specs=[VMEM] * (count + len(so_far)),
        out_specs=(VMEM,) * 3,
        input_output_aliases={count + i: i for i in range(len(so_far))},
        compiler_params=params(mib),
        cost_estimate=cost(1 << 29),
    )(normed, *pieces, *so_far)


def place_a(normed, pieces, so_far, total, whole_in, whole_down):
    mine, theirs = pieces
    c, s_mine, s_theirs = seconds()
    for slot, piece, core, second in ((0, mine, c, s_mine), (1, theirs, 1 - c, s_theirs)):
        s = along(second, 0)
        total[slot] = part(normed, piece, core, s)
        put_in(piece, core, s, whole_in)
    put_down((mine,), (theirs,), ((0, 0),), whole_down)


def place_b(normed, pieces, so_far, total, whole_in, whole_down):
    mine, theirs = pieces[:2], pieces[2:]
    c, s_mine, s_theirs = seconds()
    for slot, piece, core, second in (
        (0, mine[1], c, s_mine),
        (1, theirs[1], 1 - c, s_theirs),
    ):
        s = along(second, 1)
        total[slot] += part(normed, piece, core, s)
        put_in(piece, core, s, whole_in)
    put_down(mine, theirs, ((0, 1), (1, 0), (1, 1)), whole_down)


def place_c(normed, pieces, so_far, total, whole_in, whole_down):
    mine, theirs = pieces[:4], pieces[4:]
    c, s_mine, s_theirs = seconds()
    for slot, piece, core, s in (
        (0, mine[2], c, along(s_mine, 2)),
        (0, mine[3], c, along(s_mine, 3)),
        (1, theirs[2], 1 - c, along(s_theirs, 2)),
    ):
        total[slot] += part(normed, piece, core, s)
        put_in(piece, core, s, whole_in)
    pairs = [(k, j) for k in range(4) for j in range(3) if k > 1 or j > 1]
    put_down(mine, theirs, pairs, whole_down)


def mixer_kernel(tokens, halo, norm_gain, pool_gain, left, *refs):
    mine, theirs = refs[:4], (None, None, None, refs[4])
    out, total, whole_in, whole_down = refs[-10:-6]
    extended, pooled, middle, scaled, last, sems = refs[-6:]
    c, _, s_theirs = seconds()
    s = along(s_theirs, 3)
    put_in(theirs[3], 1 - c, s, whole_in)
    put_down(mine, theirs, [(k, 3) for k in range(4)], whole_down)
    rows = left.shape[0]
    extended[:PAD] = jnp.zeros((PAD, 512), F32)
    row = lax.broadcasted_iota(jnp.int32, (rows, 128), 0)
    lane = lax.broadcasted_iota(jnp.int32, (rows, 128), 1)
    position = lax.axis_index("sp") * 384 - HALO + row + 1
    position = jnp.maximum(position, 1).astype(F32)
    width = jnp.where(
        lane < 64, jnp.where(lane < 32, 2.0, 4.0), jnp.where(lane < 96, 8.0, 16.0)
    )
    count = jnp.minimum(position, width)

    def rounded(block):
        return block.astype(BF16).astype(F32)

    def pool(l):
        for j in range(4):
            lanes = slice(j * 128, (j + 1) * 128)
            own = extended[:, lanes]
            two = own + pltpu.roll(own, 1, 0)
            four = two + pltpu.roll(two, 2, 0)
            eight = four + pltpu.roll(four, 4, 0)
            sixteen = eight + pltpu.roll(eight, 8, 0)
            sums = jnp.where(
                lane < 64,
                jnp.where(lane < 32, two[PAD:], four[PAD:]),
                jnp.where(lane < 96, eight[PAD:], sixteen[PAD:]),
            )
            trailing = sums / count - own[PAD:]
            pooled[:, lanes] = (trailing * pool_gain[l : l + 1, lanes]).astype(BF16)

    extended[PAD:, pl.ds(pl.multiple_of(c * 256, 256), 256)] = rounded(total[0])
    extended[PAD:, pl.ds(pl.multiple_of((1 - c) * 256, 256), 256)] = rounded(
        total[1] + part(left, theirs[3], 1 - c, s)
    )
    pool(0)
    squares = jnp.zeros((rows, 128), F32)
    for j in range(4):
        lanes = slice(j * 512, (j + 1) * 512)
        down = jnp.dot(
            pooled[...],
            whole_down[0, :, :, lanes].reshape(512, 512),
            preferred_element_type=F32,
        )
        before = jnp.concatenate([halo[:, lanes], tokens[:, lanes]], axis=0)
        middle[:, lanes] = (before.astype(F32) + down).astype(BF16)
        block = middle[:, lanes].astype(F32)
        scaled[:, lanes] = (block * norm_gain[1:2, lanes]).astype(BF16)
        block = block * block
        squares += (block[:, :128] + block[:, 128:256]) + (
            block[:, 256:384] + block[:, 384:]
        )
    mean = jnp.sum(squares, axis=1, keepdims=True) / 2048.0
    pool_in = lax.dot_general(
        scaled[...],
        whole_in[...].reshape(512, 2048),
        (((1,), (1,)), ((), ())),
        preferred_element_type=F32,
    )
    extended[PAD:] = rounded(pool_in * lax.rsqrt(mean + EPS))
    pool(1)
    copies = []
    for j in range(4):
        lanes = slice(j * 512, (j + 1) * 512)
        down = jnp.dot(
            pooled[HALO:],
            whole_down[1, :, :, lanes].reshape(512, 512),
            preferred_element_type=F32,
        )
        last[:, lanes] = (middle[HALO:, lanes].astype(F32) + down).astype(BF16)
        copies.append(
            pltpu.make_async_copy(last.at[:, lanes], out.at[:, lanes], sems.at[j])
        )
        copies[-1].start()
    for copy in copies:
        copy.wait()


def mixer(tokens, halo, norm_gain, pool_gain, normed, pieces, so_far):
    rows = normed.shape[0]
    at = 5 + len(pieces)
    return pl.pallas_call(
        mixer_kernel,
        out_shape=(
            jax.ShapeDtypeStruct(tokens.shape, tokens.dtype),
            jax.ShapeDtypeStruct((2, rows, 256), F32),
            *wholes(),
        ),
        in_specs=[VMEM] * (at + 3),
        out_specs=(pl.BlockSpec(memory_space=pl.ANY),) + (VMEM,) * 3,
        input_output_aliases={at: 1, at + 1: 2, at + 2: 3},
        scratch_shapes=[
            pltpu.VMEM((PAD + rows, 512), F32),
            pltpu.VMEM((rows, 512), BF16),
            pltpu.VMEM((rows, 2048), BF16),
            pltpu.VMEM((rows, 2048), BF16),
            pltpu.VMEM(tokens.shape, BF16),
            pltpu.SemaphoreType.DMA((4,)),
        ],
        compiler_params=params(16),
        cost_estimate=cost(4 << 30),
        name="mixer",
    )(tokens, halo, norm_gain, pool_gain, normed, *pieces, *so_far)[0]


def mixed(tokens, norm_gain, in_weight, down_weight, pool_gain):
    rows = tokens.shape[1]
    halo = lax.ppermute(
        tokens[0, rows - HALO :], AXES, [(i, i + 32) for i in range(480)]
    )
    normed, pool_gain = head(halo, tokens[0], norm_gain, pool_gain)
    column = shared(packed(in_weight, down_weight), lambda y, x, z, c: (y, x, c))
    line = shared(
        jnp.broadcast_to(column[None], (4, 16, 64, 128)),
        lambda y, x, z, c: (y, z, c) if c == 0 else (x, z, c),
    )
    names = (2, -1, 1)
    mine = [line] + [send(line, second_hop(d)) for d in names]
    theirs = [send(piece, other_core) for piece in mine]
    so_far = placed(place_a, 10, normed, mine[:1] + theirs[:1], ())
    so_far = placed(place_b, 10, normed, mine[:2] + theirs[:2], so_far)
    so_far = placed(place_c, 12, normed, mine + theirs[:3], so_far)
    return mixer(
        tokens[0], halo, norm_gain, pool_gain, normed, mine + theirs[3:], so_far
    )[None]


def solution(mesh):
    in_specs = (P("tp", "sp", None), P(), P(None, "sp", "tp"), P(None, "sp", "tp"), P())
    out_specs = P("tp", "sp", None)
    return jax.shard_map(
        mixed, mesh=mesh, in_specs=in_specs, out_specs=out_specs, check_vma=False
    )
```

```python
import jax
import jax.numpy as jnp
from jax import lax
from jax.experimental import pallas as pl
from jax.experimental.pallas import tpu as pltpu
from jax.sharding import PartitionSpec as P

EPS = 1e-06
HALO = 32
PAD = 16
AXES = ("sp", "tp")
PIECES = (0, 2, 1, -1)
VMEM = pl.BlockSpec(memory_space=pltpu.VMEM)
BF16, F32 = jnp.bfloat16, jnp.float32


def number(y, x, z, c):
    return (((y % 4) * 4 + x % 4) * 16 + z % 16) * 2 + c


def places():
    for i in range(512):
        yield i, (i // 128, i // 32 % 4, i // 2 % 16, i % 2)


def send(block, target):
    route = [(i, number(*target(*place))) for i, place in places()]
    return lax.ppermute(block, AXES, route)


def shared(copies, key):
    groups = {}
    for i, place in places():
        groups.setdefault(key(*place), []).append(i)
    return lax.all_to_all(
        copies, AXES, 0, 0, axis_index_groups=list(groups.values()), tiled=True
    )


def second_hop(d):
    return lambda y, x, z, c: (y + d, x, z, c) if c == 0 else (y, x + d, z, c)


def other_core(y, x, z, c):
    return y, x, z, 1 - c


def seconds():
    sp, c = lax.axis_index("sp"), lax.axis_index("tp") % 2
    y, x = sp // 4, sp % 4
    return c, jnp.where(c == 0, y, x), jnp.where(c == 0, x, y)


def lanes_of(core, s, f):
    at = jnp.where(core == 0, s * 4 + f, f * 4 + s)
    return pl.ds(pl.multiple_of(at * 128, 128), 128)


def along(second, k):
    return (second + PIECES[k] + 4) % 4


def part(left, piece, core, s):
    lhs = jnp.concatenate([left[:, lanes_of(core, s, f)] for f in range(4)], axis=1)
    rhs = jnp.concatenate(
        [piece[f, :, 0:16].reshape(256, 128) for f in range(4)], axis=1
    )
    return lax.dot_general(
        lhs, rhs, (((1,), (1,)), ((), ())), preferred_element_type=F32
    )


def put_in(piece, core, s, whole_in):
    def step(f, carry):
        whole_in[core, :, :, lanes_of(core, s, f)] = piece[f, :, 16:32]
        return carry

    lax.fori_loop(0, 4, step, 0)


def put_down(mine, theirs, pairs, whole_down):
    c, s_mine, s_theirs = seconds()
    left = (lax.broadcasted_iota(jnp.int32, (32, 128), 1) < 64) ^ (c == 1)
    for k, j in pairs:
        a, b = along(s_mine, k), along(s_theirs, j)
        at = jnp.where(c == 0, a * 4 + b, b * 4 + a)
        rows = pl.ds(pl.multiple_of(at * 16, 16), 16)
        for z in range(16):
            m = mine[k][b, z, 32:64]
            t = theirs[j][a, z, 32:64]
            lanes = slice(z * 128, (z + 1) * 128)
            first = jnp.where(left, m, t)
            last = jnp.where(left, t, m)
            last = jnp.concatenate([last[:, 64:], last[:, :64]], axis=1)
            for l, tile in enumerate((first, last)):
                whole_down[l, 0, rows, lanes] = tile[:16]
                whole_down[l, 1, rows, lanes] = tile[16:]


def params(mib):
    return pltpu.CompilerParams(vmem_limit_bytes=mib << 20)


def cost(flops):
    return pl.CostEstimate(flops=flops, bytes_accessed=1 << 20, transcendentals=0)


def packed(in_weight, down_weight):
    core = lax.axis_index("tp") % 2
    turned = jnp.swapaxes(in_weight, 1, 2).reshape(32, 128)
    first = jnp.where(core == 0, down_weight[0], down_weight[1])
    last = jnp.where(core == 0, down_weight[1], down_weight[0])
    folded = jnp.concatenate([first, last], axis=1)
    block = jnp.concatenate([turned, folded], axis=0)
    return jnp.broadcast_to(block[None], (16, 64, 128))


def end_kernel(tokens, end):
    end[...] = tokens[tokens.shape[0] - HALO :]


def end_of(tokens):
    return pl.pallas_call(
        end_kernel,
        out_shape=jax.ShapeDtypeStruct((HALO, tokens.shape[1]), BF16),
        in_specs=[VMEM],
        out_specs=VMEM,
        compiler_params=params(3),
        cost_estimate=cost(1 << 20),
        name="end",
    )(tokens)


def head_kernel(halo, tokens, norm_gain, pool_gain, normed, gain_out):
    gain = norm_gain[0:1]

    def norm_rows(block):
        residual = block.astype(F32)
        mean = jnp.mean(residual * residual, axis=1, keepdims=True)
        return (residual * lax.rsqrt(mean + EPS) * gain).astype(BF16)

    def norm(i, carry):
        rows = pl.multiple_of(i * 32, 32)
        normed[pl.ds(HALO + rows, 32)] = norm_rows(tokens[pl.ds(rows, 32)])
        return carry

    lax.fori_loop(0, tokens.shape[0] // 32, norm, 0)
    normed[:HALO] = norm_rows(halo[...])
    old = lax.broadcasted_iota(jnp.int32, (512, 512), 0)
    new = lax.broadcasted_iota(jnp.int32, (512, 512), 1)
    source = new % 256 // 16 * 32 + new // 256 * 16 + new % 16
    gain_out[...] = jnp.dot(
        pool_gain[...],
        (old == source).astype(F32),
        precision=lax.Precision.HIGHEST,
        preferred_element_type=F32,
    )


def head(halo, tokens, norm_gain, pool_gain):
    return pl.pallas_call(
        head_kernel,
        out_shape=(
            jax.ShapeDtypeStruct((HALO + tokens.shape[0], 2048), BF16),
            jax.ShapeDtypeStruct(pool_gain.shape, F32),
        ),
        in_specs=[VMEM] * 4,
        out_specs=(VMEM, VMEM),
        compiler_params=params(5),
        cost_estimate=cost(1 << 30),
        name="head",
    )(halo, tokens, norm_gain, pool_gain)


def wholes():
    return (
        jax.ShapeDtypeStruct((2, 16, 16, 2048), BF16),
        jax.ShapeDtypeStruct((2, 2, 256, 2048), BF16),
    )


def placed(body, mib, normed, pieces, so_far):
    rows = normed.shape[0]
    count = 1 + len(pieces)

    def kernel(*refs):
        body(refs[0], refs[1:count], refs[count:-3], *refs[-3:])

    return pl.pallas_call(
        kernel,
        out_shape=(jax.ShapeDtypeStruct((2, rows, 256), F32), *wholes()),
        in_specs=[VMEM] * (count + len(so_far)),
        out_specs=(VMEM,) * 3,
        input_output_aliases={count + i: i for i in range(len(so_far))},
        compiler_params=params(mib),
        cost_estimate=cost(1 << 29),
    )(normed, *pieces, *so_far)


def place_a(normed, pieces, so_far, total, whole_in, whole_down):
    mine, theirs = pieces
    c, s_mine, s_theirs = seconds()
    for slot, piece, core, second in ((0, mine, c, s_mine), (1, theirs, 1 - c, s_theirs)):
        s = along(second, 0)
        total[slot] = part(normed, piece, core, s)
        put_in(piece, core, s, whole_in)
    put_down((mine,), (theirs,), ((0, 0),), whole_down)


def place_b(normed, pieces, so_far, total, whole_in, whole_down):
    mine, theirs = pieces[:2], pieces[2:]
    c, s_mine, s_theirs = seconds()
    for slot, piece, core, second in (
        (0, mine[1], c, s_mine),
        (1, theirs[1], 1 - c, s_theirs),
    ):
        s = along(second, 1)
        total[slot] += part(normed, piece, core, s)
        put_in(piece, core, s, whole_in)
    put_down(mine, theirs, ((0, 1), (1, 0), (1, 1)), whole_down)


def place_c(normed, pieces, so_far, total, whole_in, whole_down):
    mine, theirs = pieces[:4], pieces[4:]
    c, s_mine, s_theirs = seconds()
    for slot, piece, core, s in (
        (0, mine[2], c, along(s_mine, 2)),
        (0, mine[3], c, along(s_mine, 3)),
        (1, theirs[2], 1 - c, along(s_theirs, 2)),
    ):
        total[slot] += part(normed, piece, core, s)
        put_in(piece, core, s, whole_in)
    pairs = [(k, j) for k in range(4) for j in range(3) if k > 1 or j > 1]
    put_down(mine, theirs, pairs, whole_down)


def mixer_kernel(tokens, halo, norm_gain, pool_gain, left, *refs):
    mine, theirs = refs[:4], (None, None, None, refs[4])
    out, total, whole_in, whole_down = refs[-10:-6]
    extended, pooled, middle, scaled, last, sems = refs[-6:]
    c, _, s_theirs = seconds()
    s = along(s_theirs, 3)
    put_in(theirs[3], 1 - c, s, whole_in)
    put_down(mine, theirs, [(k, 3) for k in range(4)], whole_down)
    rows = left.shape[0]
    extended[:PAD] = jnp.zeros((PAD, 512), F32)
    row = lax.broadcasted_iota(jnp.int32, (rows, 128), 0)
    lane = lax.broadcasted_iota(jnp.int32, (rows, 128), 1)
    position = lax.axis_index("sp") * 384 - HALO + row + 1
    position = jnp.maximum(position, 1).astype(F32)
    width = jnp.where(
        lane < 64, jnp.where(lane < 32, 2.0, 4.0), jnp.where(lane < 96, 8.0, 16.0)
    )
    count = jnp.minimum(position, width)

    def rounded(block):
        return block.astype(BF16).astype(F32)

    def pool(l):
        for j in range(4):
            lanes = slice(j * 128, (j + 1) * 128)
            own = extended[:, lanes]
            two = own + pltpu.roll(own, 1, 0)
            four = two + pltpu.roll(two, 2, 0)
            eight = four + pltpu.roll(four, 4, 0)
            sixteen = eight + pltpu.roll(eight, 8, 0)
            sums = jnp.where(
                lane < 64,
                jnp.where(lane < 32, two[PAD:], four[PAD:]),
                jnp.where(lane < 96, eight[PAD:], sixteen[PAD:]),
            )
            trailing = sums / count - own[PAD:]
            pooled[:, lanes] = (trailing * pool_gain[l : l + 1, lanes]).astype(BF16)

    extended[PAD:, pl.ds(pl.multiple_of(c * 256, 256), 256)] = rounded(total[0])
    extended[PAD:, pl.ds(pl.multiple_of((1 - c) * 256, 256), 256)] = rounded(
        total[1] + part(left, theirs[3], 1 - c, s)
    )
    pool(0)
    squares = jnp.zeros((rows, 128), F32)
    for j in range(4):
        lanes = slice(j * 512, (j + 1) * 512)
        down = jnp.dot(
            pooled[...],
            whole_down[0, :, :, lanes].reshape(512, 512),
            preferred_element_type=F32,
        )
        before = jnp.concatenate([halo[:, lanes], tokens[:, lanes]], axis=0)
        middle[:, lanes] = (before.astype(F32) + down).astype(BF16)
        block = middle[:, lanes].astype(F32)
        scaled[:, lanes] = (block * norm_gain[1:2, lanes]).astype(BF16)
        block = block * block
        squares += (block[:, :128] + block[:, 128:256]) + (
            block[:, 256:384] + block[:, 384:]
        )
    mean = jnp.sum(squares, axis=1, keepdims=True) / 2048.0
    pool_in = lax.dot_general(
        scaled[...],
        whole_in[...].reshape(512, 2048),
        (((1,), (1,)), ((), ())),
        preferred_element_type=F32,
    )
    extended[PAD:] = rounded(pool_in * lax.rsqrt(mean + EPS))
    pool(1)
    copies = []
    for j in range(4):
        lanes = slice(j * 512, (j + 1) * 512)
        down = jnp.dot(
            pooled[HALO:],
            whole_down[1, :, :, lanes].reshape(512, 512),
            preferred_element_type=F32,
        )
        last[:, lanes] = (middle[HALO:, lanes].astype(F32) + down).astype(BF16)
        copies.append(
            pltpu.make_async_copy(last.at[:, lanes], out.at[:, lanes], sems.at[j])
        )
        copies[-1].start()
    for copy in copies:
        copy.wait()


def mixer(tokens, halo, norm_gain, pool_gain, normed, pieces, so_far):
    rows = normed.shape[0]
    at = 5 + len(pieces)
    return pl.pallas_call(
        mixer_kernel,
        out_shape=(
            jax.ShapeDtypeStruct(tokens.shape, tokens.dtype),
            jax.ShapeDtypeStruct((2, rows, 256), F32),
            *wholes(),
        ),
        in_specs=[VMEM] * (at + 3),
        out_specs=(pl.BlockSpec(memory_space=pl.ANY),) + (VMEM,) * 3,
        input_output_aliases={at: 1, at + 1: 2, at + 2: 3},
        scratch_shapes=[
            pltpu.VMEM((PAD + rows, 512), F32),
            pltpu.VMEM((rows, 512), BF16),
            pltpu.VMEM((rows, 2048), BF16),
            pltpu.VMEM((rows, 2048), BF16),
            pltpu.VMEM(tokens.shape, BF16),
            pltpu.SemaphoreType.DMA((4,)),
        ],
        compiler_params=params(16),
        cost_estimate=cost(4 << 30),
        name="mixer",
    )(tokens, halo, norm_gain, pool_gain, normed, *pieces, *so_far)[0]


def mixed(tokens, norm_gain, in_weight, down_weight, pool_gain):
    end = end_of(tokens[0])
    halo = lax.ppermute(end, AXES, [(i, i + 32) for i in range(480)])
    normed, pool_gain = head(halo, tokens[0], norm_gain, pool_gain)
    column = shared(packed(in_weight, down_weight), lambda y, x, z, c: (y, x, c))
    line = shared(
        jnp.broadcast_to(column[None], (4, 16, 64, 128)),
        lambda y, x, z, c: (y, z, c) if c == 0 else (x, z, c),
    )
    names = (2, -1, 1)
    mine = [line] + [send(line, second_hop(d)) for d in names]
    theirs = [send(piece, other_core) for piece in mine]
    so_far = placed(place_a, 10, normed, mine[:1] + theirs[:1], ())
    so_far = placed(place_b, 10, normed, mine[:2] + theirs[:2], so_far)
    so_far = placed(place_c, 12, normed, mine + theirs[:3], so_far)
    return mixer(
        tokens[0], halo, norm_gain, pool_gain, normed, mine + theirs[3:], so_far
    )[None]


def solution(mesh):
    in_specs = (P("tp", "sp", None), P(), P(None, "sp", "tp"), P(None, "sp", "tp"), P())
    out_specs = P("tp", "sp", None)
    return jax.shard_map(
        mixed, mesh=mesh, in_specs=in_specs, out_specs=out_specs, check_vma=False
    )
```

```python
import jax
import jax.numpy as jnp
from jax import lax
from jax.experimental import pallas as pl
from jax.experimental.pallas import tpu as pltpu
from jax.sharding import PartitionSpec as P

EPS = 1e-06
HALO = 32
PAD = 16
AXES = ("sp", "tp")
PIECES = (0, -1, 1, 2)
VMEM = pl.BlockSpec(memory_space=pltpu.VMEM)
BF16, F32 = jnp.bfloat16, jnp.float32


def number(y, x, z, c):
    return (((y % 4) * 4 + x % 4) * 16 + z % 16) * 2 + c


def places():
    for i in range(512):
        yield i, (i // 128, i // 32 % 4, i // 2 % 16, i % 2)


def send(block, target):
    route = [(i, number(*target(*place))) for i, place in places()]
    return lax.ppermute(block, AXES, route)


def shared(copies, key):
    groups = {}
    for i, place in places():
        groups.setdefault(key(*place), []).append(i)
    return lax.all_to_all(
        copies, AXES, 0, 0, axis_index_groups=list(groups.values()), tiled=True
    )


def second_hop(d):
    return lambda y, x, z, c: (y + d, x, z, c) if c == 0 else (y, x + d, z, c)


def other_core(y, x, z, c):
    return y, x, z, 1 - c


def seconds():
    sp, c = lax.axis_index("sp"), lax.axis_index("tp") % 2
    y, x = sp // 4, sp % 4
    return c, jnp.where(c == 0, y, x), jnp.where(c == 0, x, y)


def lanes_of(core, s, f):
    at = jnp.where(core == 0, s * 4 + f, f * 4 + s)
    return pl.ds(pl.multiple_of(at * 128, 128), 128)


def along(second, k):
    return (second + PIECES[k] + 4) % 4


def part(left, rows, piece, core, s):
    lhs = jnp.concatenate([left[rows, lanes_of(core, s, f)] for f in range(4)], axis=1)
    rhs = jnp.concatenate(
        [piece[f, :, 0:16].reshape(256, 128) for f in range(4)], axis=1
    )
    return lax.dot_general(
        lhs, rhs, (((1,), (1,)), ((), ())), preferred_element_type=F32
    )


def put_in(piece, core, s, whole_in):
    def step(f, carry):
        whole_in[core, :, :, lanes_of(core, s, f)] = piece[f, :, 16:32]
        return carry

    lax.fori_loop(0, 4, step, 0)


def put_down(mine, theirs, pairs, whole_down):
    c, s_mine, s_theirs = seconds()
    left = (lax.broadcasted_iota(jnp.int32, (32, 128), 1) < 64) ^ (c == 1)
    for k, j in pairs:
        a, b = along(s_mine, k), along(s_theirs, j)
        at = jnp.where(c == 0, a * 4 + b, b * 4 + a)
        rows = pl.ds(pl.multiple_of(at * 16, 16), 16)
        for z in range(16):
            m = mine[k][b, z, 32:64]
            t = theirs[j][a, z, 32:64]
            lanes = slice(z * 128, (z + 1) * 128)
            first = jnp.where(left, m, t)
            last = jnp.where(left, t, m)
            last = jnp.concatenate([last[:, 64:], last[:, :64]], axis=1)
            for l, tile in enumerate((first, last)):
                whole_down[l, 0, rows, lanes] = tile[:16]
                whole_down[l, 1, rows, lanes] = tile[16:]


def params(mib):
    return pltpu.CompilerParams(vmem_limit_bytes=mib << 20)


def cost(flops):
    return pl.CostEstimate(flops=flops, bytes_accessed=1 << 20, transcendentals=0)


def packed(in_weight, down_weight):
    core = lax.axis_index("tp") % 2
    turned = jnp.swapaxes(in_weight, 1, 2).reshape(32, 128)
    first = jnp.where(core == 0, down_weight[0], down_weight[1])
    last = jnp.where(core == 0, down_weight[1], down_weight[0])
    folded = jnp.concatenate([first, last], axis=1)
    block = jnp.concatenate([turned, folded], axis=0)
    return jnp.broadcast_to(block[None], (16, 64, 128))


def end_kernel(tokens, end):
    end[...] = tokens[tokens.shape[0] - HALO :]


def end_of(tokens):
    return pl.pallas_call(
        end_kernel,
        out_shape=jax.ShapeDtypeStruct((HALO, tokens.shape[1]), BF16),
        in_specs=[VMEM],
        out_specs=VMEM,
        compiler_params=params(3),
        cost_estimate=cost(1 << 20),
        name="end",
    )(tokens)


def norm_rows(block, gain):
    residual = block.astype(F32)
    mean = jnp.mean(residual * residual, axis=1, keepdims=True)
    return (residual * lax.rsqrt(mean + EPS) * gain).astype(BF16)


def head_kernel(tokens, norm_gain, pool_gain, normed, gain_out):
    def norm(i, carry):
        rows = pl.multiple_of(i * 32, 32)
        normed[pl.ds(HALO + rows, 32)] = norm_rows(
            tokens[pl.ds(rows, 32)], norm_gain[0:1]
        )
        return carry

    lax.fori_loop(0, tokens.shape[0] // 32, norm, 0)
    old = lax.broadcasted_iota(jnp.int32, (512, 512), 0)
    new = lax.broadcasted_iota(jnp.int32, (512, 512), 1)
    source = new % 256 // 16 * 32 + new // 256 * 16 + new % 16
    gain_out[...] = jnp.dot(
        pool_gain[...],
        (old == source).astype(F32),
        precision=lax.Precision.HIGHEST,
        preferred_element_type=F32,
    )


def head(tokens, norm_gain, pool_gain):
    return pl.pallas_call(
        head_kernel,
        out_shape=(
            jax.ShapeDtypeStruct((HALO + tokens.shape[0], 2048), BF16),
            jax.ShapeDtypeStruct(pool_gain.shape, F32),
        ),
        in_specs=[VMEM] * 3,
        out_specs=(VMEM, VMEM),
        compiler_params=params(5),
        cost_estimate=cost(1 << 30),
        name="head",
    )(tokens, norm_gain, pool_gain)


def wholes():
    return (
        jax.ShapeDtypeStruct((2, 16, 16, 2048), BF16),
        jax.ShapeDtypeStruct((2, 2, 256, 2048), BF16),
    )


def placed(body, mib, inputs, state):
    rows = state[0].shape[0]
    count = len(inputs)

    def kernel(*refs):
        body(refs[:count], *refs[-4:])

    return pl.pallas_call(
        kernel,
        out_shape=(
            jax.ShapeDtypeStruct((rows, 2048), BF16),
            jax.ShapeDtypeStruct((2, rows, 256), F32),
            *wholes(),
        ),
        in_specs=[VMEM] * (count + len(state)),
        out_specs=(VMEM,) * 4,
        input_output_aliases={count + i: i for i in range(len(state))},
        compiler_params=params(mib),
        cost_estimate=cost(1 << 29),
    )(*inputs, *state)


def place_a(inputs, normed, total, whole_in, whole_down):
    mine, theirs = inputs
    c, s_mine, s_theirs = seconds()
    for slot, piece, core, second in ((0, mine, c, s_mine), (1, theirs, 1 - c, s_theirs)):
        s = along(second, 0)
        rows = slice(HALO, None)
        total[slot, rows] = part(normed, rows, piece, core, s)
        put_in(piece, core, s, whole_in)
    put_down((mine,), (theirs,), ((0, 0),), whole_down)


def place_b(inputs, normed, total, whole_in, whole_down):
    halo, norm_gain, *pieces = inputs
    mine, theirs = pieces[:3], pieces[3:]
    normed[:HALO] = norm_rows(halo[...], norm_gain[0:1])
    c, s_mine, s_theirs = seconds()
    for slot, of, core, second in ((0, mine, c, s_mine), (1, theirs, 1 - c, s_theirs)):
        rows = slice(0, HALO)
        total[slot, rows] = part(normed, rows, of[0], core, along(second, 0))
        for k in (1, 2):
            s = along(second, k)
            total[slot] += part(normed, slice(None), of[k], core, s)
            put_in(of[k], core, s, whole_in)
    pairs = [(k, j) for k in range(3) for j in range(3) if k + j > 0]
    put_down(mine, theirs, pairs, whole_down)


def place_c(inputs, normed, total, whole_in, whole_down):
    mine, theirs = (None, None, None, inputs[0]), inputs[1:]
    c, s_mine, _ = seconds()
    s = along(s_mine, 3)
    total[0] += part(normed, slice(None), mine[3], c, s)
    put_in(mine[3], c, s, whole_in)
    put_down(mine, theirs, [(3, j) for j in range(3)], whole_down)


def mixer_kernel(tokens, halo, norm_gain, pool_gain, *refs):
    mine, theirs, left = refs[:4], (None, None, None, refs[4]), refs[5]
    out, total, whole_in, whole_down = refs[-10:-6]
    extended, pooled, middle, scaled, last, sems = refs[-6:]
    c, _, s_theirs = seconds()
    s = along(s_theirs, 3)
    put_in(theirs[3], 1 - c, s, whole_in)
    put_down(mine, theirs, [(k, 3) for k in range(4)], whole_down)
    rows = left.shape[0]
    extended[:PAD] = jnp.zeros((PAD, 512), F32)
    row = lax.broadcasted_iota(jnp.int32, (rows, 128), 0)
    lane = lax.broadcasted_iota(jnp.int32, (rows, 128), 1)
    position = lax.axis_index("sp") * 384 - HALO + row + 1
    position = jnp.maximum(position, 1).astype(F32)
    width = jnp.where(
        lane < 64, jnp.where(lane < 32, 2.0, 4.0), jnp.where(lane < 96, 8.0, 16.0)
    )
    count = jnp.minimum(position, width)

    def rounded(block):
        return block.astype(BF16).astype(F32)

    def pool(l):
        for j in range(4):
            lanes = slice(j * 128, (j + 1) * 128)
            own = extended[:, lanes]
            two = own + pltpu.roll(own, 1, 0)
            four = two + pltpu.roll(two, 2, 0)
            eight = four + pltpu.roll(four, 4, 0)
            sixteen = eight + pltpu.roll(eight, 8, 0)
            sums = jnp.where(
                lane < 64,
                jnp.where(lane < 32, two[PAD:], four[PAD:]),
                jnp.where(lane < 96, eight[PAD:], sixteen[PAD:]),
            )
            trailing = sums / count - own[PAD:]
            pooled[:, lanes] = (trailing * pool_gain[l : l + 1, lanes]).astype(BF16)

    extended[PAD:, pl.ds(pl.multiple_of(c * 256, 256), 256)] = rounded(total[0])
    extended[PAD:, pl.ds(pl.multiple_of((1 - c) * 256, 256), 256)] = rounded(
        total[1] + part(left, slice(None), theirs[3], 1 - c, s)
    )
    pool(0)
    squares = jnp.zeros((rows, 128), F32)
    for j in range(4):
        lanes = slice(j * 512, (j + 1) * 512)
        down = jnp.dot(
            pooled[...],
            whole_down[0, :, :, lanes].reshape(512, 512),
            preferred_element_type=F32,
        )
        before = jnp.concatenate([halo[:, lanes], tokens[:, lanes]], axis=0)
        middle[:, lanes] = (before.astype(F32) + down).astype(BF16)
        block = middle[:, lanes].astype(F32)
        scaled[:, lanes] = (block * norm_gain[1:2, lanes]).astype(BF16)
        block = block * block
        squares += (block[:, :128] + block[:, 128:256]) + (
            block[:, 256:384] + block[:, 384:]
        )
    mean = jnp.sum(squares, axis=1, keepdims=True) / 2048.0
    pool_in = lax.dot_general(
        scaled[...],
        whole_in[...].reshape(512, 2048),
        (((1,), (1,)), ((), ())),
        preferred_element_type=F32,
    )
    extended[PAD:] = rounded(pool_in * lax.rsqrt(mean + EPS))
    pool(1)
    copies = []
    for j in range(4):
        lanes = slice(j * 512, (j + 1) * 512)
        down = jnp.dot(
            pooled[HALO:],
            whole_down[1, :, :, lanes].reshape(512, 512),
            preferred_element_type=F32,
        )
        last[:, lanes] = (middle[HALO:, lanes].astype(F32) + down).astype(BF16)
        copies.append(
            pltpu.make_async_copy(last.at[:, lanes], out.at[:, lanes], sems.at[j])
        )
        copies[-1].start()
    for copy in copies:
        copy.wait()


def mixer(tokens, halo, norm_gain, pool_gain, pieces, state):
    rows = state[0].shape[0]
    at = 5 + len(pieces)
    return pl.pallas_call(
        mixer_kernel,
        out_shape=(
            jax.ShapeDtypeStruct(tokens.shape, tokens.dtype),
            jax.ShapeDtypeStruct((2, rows, 256), F32),
            *wholes(),
        ),
        in_specs=[VMEM] * (at + 3),
        out_specs=(pl.BlockSpec(memory_space=pl.ANY),) + (VMEM,) * 3,
        input_output_aliases={at: 1, at + 1: 2, at + 2: 3},
        scratch_shapes=[
            pltpu.VMEM((PAD + rows, 512), F32),
            pltpu.VMEM((rows, 512), BF16),
            pltpu.VMEM((rows, 2048), BF16),
            pltpu.VMEM((rows, 2048), BF16),
            pltpu.VMEM(tokens.shape, BF16),
            pltpu.SemaphoreType.DMA((4,)),
        ],
        compiler_params=params(16),
        cost_estimate=cost(4 << 30),
        name="mixer",
    )(tokens, halo, norm_gain, pool_gain, *pieces, *state)[0]


def mixed(tokens, norm_gain, in_weight, down_weight, pool_gain):
    end = end_of(tokens[0])
    halo = lax.ppermute(end, AXES, [(i, i + 32) for i in range(480)])
    normed, pool_gain = head(tokens[0], norm_gain, pool_gain)
    column = shared(packed(in_weight, down_weight), lambda y, x, z, c: (y, x, c))
    line = shared(
        jnp.broadcast_to(column[None], (4, 16, 64, 128)),
        lambda y, x, z, c: (y, z, c) if c == 0 else (x, z, c),
    )
    names = (1, -1, 2)
    mine = [line] + [send(line, second_hop(d)) for d in names]
    theirs = [send(piece, other_core) for piece in mine]
    state = placed(place_a, 10, mine[:1] + theirs[:1], (normed,))
    inputs = [halo, norm_gain, *mine[:3], *theirs[:3]]
    state = placed(place_b, 10, inputs, state)
    state = placed(place_c, 10, mine[3:] + theirs[:3], state)
    pieces = mine + theirs[3:]
    return mixer(tokens[0], halo, norm_gain, pool_gain, pieces, state)[None]


def solution(mesh):
    in_specs = (P("tp", "sp", None), P(), P(None, "sp", "tp"), P(None, "sp", "tp"), P())
    out_specs = P("tp", "sp", None)
    return jax.shard_map(
        mixed, mesh=mesh, in_specs=in_specs, out_specs=out_specs, check_vma=False
    )
```

```python
import jax
import jax.numpy as jnp
from jax import lax
from jax.experimental import pallas as pl
from jax.experimental.pallas import tpu as pltpu
from jax.sharding import PartitionSpec as P

EPS = 1e-06
HALO = 32
PAD = 16
AXES = ("sp", "tp")
PIECES = (0, -1, 1, 2)
VMEM = pl.BlockSpec(memory_space=pltpu.VMEM)
BF16, F32 = jnp.bfloat16, jnp.float32


def number(y, x, z, c):
    return (((y % 4) * 4 + x % 4) * 16 + z % 16) * 2 + c


def places():
    for i in range(512):
        yield i, (i // 128, i // 32 % 4, i // 2 % 16, i % 2)


def send(block, target):
    route = [(i, number(*target(*place))) for i, place in places()]
    return lax.ppermute(block, AXES, route)


def shared(copies, key):
    groups = {}
    for i, place in places():
        groups.setdefault(key(*place), []).append(i)
    return lax.all_to_all(
        copies, AXES, 0, 0, axis_index_groups=list(groups.values()), tiled=True
    )


def second_hop(d):
    return lambda y, x, z, c: (y + d, x, z, c) if c == 0 else (y, x + d, z, c)


def other_core(y, x, z, c):
    return y, x, z, 1 - c


def seconds():
    sp, c = lax.axis_index("sp"), lax.axis_index("tp") % 2
    y, x = sp // 4, sp % 4
    return c, jnp.where(c == 0, y, x), jnp.where(c == 0, x, y)


def lanes_of(core, s, f):
    at = jnp.where(core == 0, s * 4 + f, f * 4 + s)
    return pl.ds(pl.multiple_of(at * 128, 128), 128)


def along(second, k):
    return (second + PIECES[k] + 4) % 4


def of_first(piece, f):
    return piece[f // 2].at[f % 2] if isinstance(piece, tuple) else piece.at[f]


def down_tile(piece, f, z):
    if not isinstance(piece, tuple):
        return piece[f, z, 32:64]
    low, high = (half[f % 2, z, 32:64] for half in piece)
    return jnp.where(f < 2, low, high)


def part(left, rows, piece, core, s):
    lhs = jnp.concatenate([left[rows, lanes_of(core, s, f)] for f in range(4)], axis=1)
    rhs = jnp.concatenate(
        [of_first(piece, f)[:, 0:16].reshape(256, 128) for f in range(4)], axis=1
    )
    return lax.dot_general(
        lhs, rhs, (((1,), (1,)), ((), ())), preferred_element_type=F32
    )


def put_in(piece, core, s, whole_in):
    for f in range(4):
        whole_in[core, :, :, lanes_of(core, s, f)] = of_first(piece, f)[:, 16:32]


def put_down(mine, theirs, pairs, whole_down):
    c, s_mine, s_theirs = seconds()
    left = (lax.broadcasted_iota(jnp.int32, (32, 128), 1) < 64) ^ (c == 1)
    for k, j in pairs:
        a, b = along(s_mine, k), along(s_theirs, j)
        at = jnp.where(c == 0, a * 4 + b, b * 4 + a)
        rows = pl.ds(pl.multiple_of(at * 16, 16), 16)
        for z in range(16):
            m = down_tile(mine[k], b, z)
            t = down_tile(theirs[j], a, z)
            lanes = slice(z * 128, (z + 1) * 128)
            first = jnp.where(left, m, t)
            last = jnp.where(left, t, m)
            last = jnp.concatenate([last[:, 64:], last[:, :64]], axis=1)
            for l, tile in enumerate((first, last)):
                whole_down[l, 0, rows, lanes] = tile[:16]
                whole_down[l, 1, rows, lanes] = tile[16:]


def params(mib):
    return pltpu.CompilerParams(vmem_limit_bytes=mib << 20)


def cost(flops):
    return pl.CostEstimate(flops=flops, bytes_accessed=1 << 20, transcendentals=0)


def packed(in_weight, down_weight):
    core = lax.axis_index("tp") % 2
    turned = jnp.swapaxes(in_weight, 1, 2).reshape(32, 128)
    first = jnp.where(core == 0, down_weight[0], down_weight[1])
    last = jnp.where(core == 0, down_weight[1], down_weight[0])
    folded = jnp.concatenate([first, last], axis=1)
    block = jnp.concatenate([turned, folded], axis=0)
    return jnp.broadcast_to(block[None], (16, 64, 128))


def cut(array, low, high):
    def kernel(array, out):
        out[...] = array[low:high]

    return pl.pallas_call(
        kernel,
        out_shape=jax.ShapeDtypeStruct((high - low, *array.shape[1:]), BF16),
        in_specs=[VMEM],
        out_specs=VMEM,
        compiler_params=params(3),
        cost_estimate=cost(1 << 20),
    )(array)


def norm_rows(block, gain):
    residual = block.astype(F32)
    mean = jnp.mean(residual * residual, axis=1, keepdims=True)
    return (residual * lax.rsqrt(mean + EPS) * gain).astype(BF16)


def head_kernel(tokens, norm_gain, pool_gain, normed, gain_out):
    def norm(i, carry):
        rows = pl.multiple_of(i * 32, 32)
        normed[pl.ds(HALO + rows, 32)] = norm_rows(
            tokens[pl.ds(rows, 32)], norm_gain[0:1]
        )
        return carry

    lax.fori_loop(0, tokens.shape[0] // 32, norm, 0)
    old = lax.broadcasted_iota(jnp.int32, (512, 512), 0)
    new = lax.broadcasted_iota(jnp.int32, (512, 512), 1)
    source = new % 256 // 16 * 32 + new // 256 * 16 + new % 16
    gain_out[...] = jnp.dot(
        pool_gain[...],
        (old == source).astype(F32),
        precision=lax.Precision.HIGHEST,
        preferred_element_type=F32,
    )


def head(tokens, norm_gain, pool_gain):
    return pl.pallas_call(
        head_kernel,
        out_shape=(
            jax.ShapeDtypeStruct((HALO + tokens.shape[0], 2048), BF16),
            jax.ShapeDtypeStruct(pool_gain.shape, F32),
        ),
        in_specs=[VMEM] * 3,
        out_specs=(VMEM, VMEM),
        compiler_params=params(5),
        cost_estimate=cost(1 << 30),
        name="head",
    )(tokens, norm_gain, pool_gain)


def wholes():
    return (
        jax.ShapeDtypeStruct((2, 16, 16, 2048), BF16),
        jax.ShapeDtypeStruct((2, 2, 256, 2048), BF16),
    )


def placed(body, mib, inputs, state):
    rows = state[0].shape[0]
    count = len(inputs)

    def kernel(*refs):
        body(refs[:count], *refs[-4:])

    return pl.pallas_call(
        kernel,
        out_shape=(
            jax.ShapeDtypeStruct((rows, 2048), BF16),
            jax.ShapeDtypeStruct((2, rows, 256), F32),
            *wholes(),
        ),
        in_specs=[VMEM] * (count + len(state)),
        out_specs=(VMEM,) * 4,
        input_output_aliases={count + i: i for i in range(len(state))},
        compiler_params=params(mib),
        cost_estimate=cost(1 << 29),
    )(*inputs, *state)


def place_a(inputs, normed, total, whole_in, whole_down):
    mine, theirs = inputs
    c, s_mine, s_theirs = seconds()
    for slot, piece, core, second in ((0, mine, c, s_mine), (1, theirs, 1 - c, s_theirs)):
        s = along(second, 0)
        rows = slice(HALO, None)
        total[slot, rows] = part(normed, rows, piece, core, s)
        put_in(piece, core, s, whole_in)
    put_down((mine,), (theirs,), ((0, 0),), whole_down)


def place_b(inputs, normed, total, whole_in, whole_down):
    halo, norm_gain, *pieces = inputs
    mine, theirs = pieces[:3], pieces[3:]
    normed[:HALO] = norm_rows(halo[...], norm_gain[0:1])
    c, s_mine, s_theirs = seconds()
    for slot, of, core, second in ((0, mine, c, s_mine), (1, theirs, 1 - c, s_theirs)):
        rows = slice(0, HALO)
        total[slot, rows] = part(normed, rows, of[0], core, along(second, 0))
        for k in (1, 2):
            s = along(second, k)
            total[slot] += part(normed, slice(None), of[k], core, s)
            put_in(of[k], core, s, whole_in)
    pairs = [(k, j) for k in range(3) for j in range(3) if k + j > 0]
    put_down(mine, theirs, pairs, whole_down)


def place_c(inputs, normed, total, whole_in, whole_down):
    mine, theirs = (None, None, None, tuple(inputs[:2])), inputs[2:]
    c, s_mine, _ = seconds()
    s = along(s_mine, 3)
    total[0] += part(normed, slice(None), mine[3], c, s)
    put_in(mine[3], c, s, whole_in)
    put_down(mine, theirs, [(3, j) for j in range(3)], whole_down)


def mixer_kernel(tokens, halo, norm_gain, pool_gain, *refs):
    mine = (*refs[:3], tuple(refs[3:5]))
    theirs, left = (None, None, None, tuple(refs[5:7])), refs[7]
    out, total, whole_in, whole_down = refs[-10:-6]
    extended, pooled, middle, scaled, last, sems = refs[-6:]
    c, _, s_theirs = seconds()
    s = along(s_theirs, 3)
    put_in(theirs[3], 1 - c, s, whole_in)
    put_down(mine, theirs, [(k, 3) for k in range(4)], whole_down)
    rows = left.shape[0]
    extended[:PAD] = jnp.zeros((PAD, 512), F32)
    row = lax.broadcasted_iota(jnp.int32, (rows, 128), 0)
    lane = lax.broadcasted_iota(jnp.int32, (rows, 128), 1)
    position = lax.axis_index("sp") * 384 - HALO + row + 1
    position = jnp.maximum(position, 1).astype(F32)
    width = jnp.where(
        lane < 64, jnp.where(lane < 32, 2.0, 4.0), jnp.where(lane < 96, 8.0, 16.0)
    )
    count = jnp.minimum(position, width)

    def rounded(block):
        return block.astype(BF16).astype(F32)

    def pool(l):
        for j in range(4):
            lanes = slice(j * 128, (j + 1) * 128)
            own = extended[:, lanes]
            two = own + pltpu.roll(own, 1, 0)
            four = two + pltpu.roll(two, 2, 0)
            eight = four + pltpu.roll(four, 4, 0)
            sixteen = eight + pltpu.roll(eight, 8, 0)
            sums = jnp.where(
                lane < 64,
                jnp.where(lane < 32, two[PAD:], four[PAD:]),
                jnp.where(lane < 96, eight[PAD:], sixteen[PAD:]),
            )
            trailing = sums / count - own[PAD:]
            pooled[:, lanes] = (trailing * pool_gain[l : l + 1, lanes]).astype(BF16)

    extended[PAD:, pl.ds(pl.multiple_of(c * 256, 256), 256)] = rounded(total[0])
    extended[PAD:, pl.ds(pl.multiple_of((1 - c) * 256, 256), 256)] = rounded(
        total[1] + part(left, slice(None), theirs[3], 1 - c, s)
    )
    pool(0)
    squares = jnp.zeros((rows, 128), F32)
    for j in range(4):
        lanes = slice(j * 512, (j + 1) * 512)
        down = jnp.dot(
            pooled[...],
            whole_down[0, :, :, lanes].reshape(512, 512),
            preferred_element_type=F32,
        )
        before = jnp.concatenate([halo[:, lanes], tokens[:, lanes]], axis=0)
        middle[:, lanes] = (before.astype(F32) + down).astype(BF16)
        block = middle[:, lanes].astype(F32)
        scaled[:, lanes] = (block * norm_gain[1:2, lanes]).astype(BF16)
        block = block * block
        squares += (block[:, :128] + block[:, 128:256]) + (
            block[:, 256:384] + block[:, 384:]
        )
    mean = jnp.sum(squares, axis=1, keepdims=True) / 2048.0
    pool_in = lax.dot_general(
        scaled[...],
        whole_in[...].reshape(512, 2048),
        (((1,), (1,)), ((), ())),
        preferred_element_type=F32,
    )
    extended[PAD:] = rounded(pool_in * lax.rsqrt(mean + EPS))
    pool(1)
    copies = []
    for j in range(4):
        lanes = slice(j * 512, (j + 1) * 512)
        down = jnp.dot(
            pooled[HALO:],
            whole_down[1, :, :, lanes].reshape(512, 512),
            preferred_element_type=F32,
        )
        last[:, lanes] = (middle[HALO:, lanes].astype(F32) + down).astype(BF16)
        copies.append(
            pltpu.make_async_copy(last.at[:, lanes], out.at[:, lanes], sems.at[j])
        )
        copies[-1].start()
    for copy in copies:
        copy.wait()


def mixer(tokens, halo, norm_gain, pool_gain, pieces, state):
    rows = state[0].shape[0]
    at = 5 + len(pieces)
    return pl.pallas_call(
        mixer_kernel,
        out_shape=(
            jax.ShapeDtypeStruct(tokens.shape, tokens.dtype),
            jax.ShapeDtypeStruct((2, rows, 256), F32),
            *wholes(),
        ),
        in_specs=[VMEM] * (at + 3),
        out_specs=(pl.BlockSpec(memory_space=pl.ANY),) + (VMEM,) * 3,
        input_output_aliases={at: 1, at + 1: 2, at + 2: 3},
        scratch_shapes=[
            pltpu.VMEM((PAD + rows, 512), F32),
            pltpu.VMEM((rows, 512), BF16),
            pltpu.VMEM((rows, 2048), BF16),
            pltpu.VMEM((rows, 2048), BF16),
            pltpu.VMEM(tokens.shape, BF16),
            pltpu.SemaphoreType.DMA((4,)),
        ],
        compiler_params=params(16),
        cost_estimate=cost(4 << 30),
        name="mixer",
    )(tokens, halo, norm_gain, pool_gain, *pieces, *state)[0]


def mixed(tokens, norm_gain, in_weight, down_weight, pool_gain):
    rows = tokens.shape[1]
    end = cut(tokens[0], rows - HALO, rows)
    halo = lax.ppermute(end, AXES, [(i, i + 32) for i in range(480)])
    normed, pool_gain = head(tokens[0], norm_gain, pool_gain)
    column = shared(packed(in_weight, down_weight), lambda y, x, z, c: (y, x, c))
    line = shared(
        jnp.broadcast_to(column[None], (4, 16, 64, 128)),
        lambda y, x, z, c: (y, z, c) if c == 0 else (x, z, c),
    )
    up = send(line, second_hop(1))
    down = send(line, second_hop(-1))
    up_on = send(cut(up, 0, 2), second_hop(1))
    down_on = send(cut(down, 2, 4), second_hop(-1))
    mine = [line, up, down, up_on, down_on]
    theirs = [send(piece, other_core) for piece in mine]
    state = placed(place_a, 10, mine[:1] + theirs[:1], (normed,))
    inputs = [halo, norm_gain, *mine[:3], *theirs[:3]]
    state = placed(place_b, 10, inputs, state)
    state = placed(place_c, 10, mine[3:] + theirs[:3], state)
    pieces = mine + theirs[3:]
    return mixer(tokens[0], halo, norm_gain, pool_gain, pieces, state)[None]


def solution(mesh):
    in_specs = (P("tp", "sp", None), P(), P(None, "sp", "tp"), P(None, "sp", "tp"), P())
    out_specs = P("tp", "sp", None)
    return jax.shard_map(
        mixed, mesh=mesh, in_specs=in_specs, out_specs=out_specs, check_vma=False
    )
```

```python
import jax
import jax.numpy as jnp
from jax import lax
from jax.experimental import pallas as pl
from jax.experimental.pallas import tpu as pltpu
from jax.sharding import PartitionSpec as P

EPS = 1e-06
HALO = 32
PAD = 16
AXES = ("sp", "tp")
PIECES = (0, -1, 1, 2)
VMEM = pl.BlockSpec(memory_space=pltpu.VMEM)
BF16, F32 = jnp.bfloat16, jnp.float32


def number(y, x, z, c):
    return (((y % 4) * 4 + x % 4) * 16 + z % 16) * 2 + c


def places():
    for i in range(512):
        yield i, (i // 128, i // 32 % 4, i // 2 % 16, i % 2)


def send(block, target):
    route = [(i, number(*target(*place))) for i, place in places()]
    return lax.ppermute(block, AXES, route)


def shared(copies, key):
    groups = {}
    for i, place in places():
        groups.setdefault(key(*place), []).append(i)
    return lax.all_to_all(
        copies, AXES, 0, 0, axis_index_groups=list(groups.values()), tiled=True
    )


def second_hop(d):
    return lambda y, x, z, c: (y + d, x, z, c) if c == 0 else (y, x + d, z, c)


def other_core(y, x, z, c):
    return y, x, z, 1 - c


def seconds():
    sp, c = lax.axis_index("sp"), lax.axis_index("tp") % 2
    y, x = sp // 4, sp % 4
    return c, jnp.where(c == 0, y, x), jnp.where(c == 0, x, y)


def lanes_of(core, s, f):
    at = jnp.where(core == 0, s * 4 + f, f * 4 + s)
    return pl.ds(pl.multiple_of(at * 128, 128), 128)


def along(second, k):
    return (second + PIECES[k] + 4) % 4


def of_first(piece, f):
    return piece[f // 2].at[f % 2] if isinstance(piece, tuple) else piece.at[f]


def down_tile(piece, f, z):
    if not isinstance(piece, tuple):
        return piece[f, z, 32:64]
    low, high = (half[f % 2, z, 32:64] for half in piece)
    return jnp.where(f < 2, low, high)


def part(left, rows, piece, core, s):
    lhs = jnp.concatenate([left[rows, lanes_of(core, s, f)] for f in range(4)], axis=1)
    rhs = jnp.concatenate(
        [of_first(piece, f)[:, 0:16].reshape(256, 128) for f in range(4)], axis=1
    )
    return lax.dot_general(
        lhs, rhs, (((1,), (1,)), ((), ())), preferred_element_type=F32
    )


def put_in(piece, core, s, whole_in):
    for f in range(4):
        whole_in[core, :, :, lanes_of(core, s, f)] = of_first(piece, f)[:, 16:32]


def put_down(mine, theirs, pairs, whole_down):
    c, s_mine, s_theirs = seconds()
    left = (lax.broadcasted_iota(jnp.int32, (32, 128), 1) < 64) ^ (c == 1)
    for k, j in pairs:
        a, b = along(s_mine, k), along(s_theirs, j)
        at = jnp.where(c == 0, a * 4 + b, b * 4 + a)
        rows = pl.ds(pl.multiple_of(at * 16, 16), 16)
        for z in range(16):
            m = down_tile(mine[k], b, z)
            t = down_tile(theirs[j], a, z)
            lanes = slice(z * 128, (z + 1) * 128)
            first = jnp.where(left, m, t)
            last = jnp.where(left, t, m)
            last = jnp.concatenate([last[:, 64:], last[:, :64]], axis=1)
            for l, tile in enumerate((first, last)):
                whole_down[l, 0, rows, lanes] = tile[:16]
                whole_down[l, 1, rows, lanes] = tile[16:]


def params(mib):
    return pltpu.CompilerParams(vmem_limit_bytes=mib << 20)


def cost(flops):
    return pl.CostEstimate(flops=flops, bytes_accessed=1 << 20, transcendentals=0)


def packed(in_weight, down_weight):
    core = lax.axis_index("tp") % 2
    turned = jnp.swapaxes(in_weight, 1, 2).reshape(32, 128)
    first = jnp.where(core == 0, down_weight[0], down_weight[1])
    last = jnp.where(core == 0, down_weight[1], down_weight[0])
    folded = jnp.concatenate([first, last], axis=1)
    block = jnp.concatenate([turned, folded], axis=0)
    return jnp.broadcast_to(block[None], (16, 64, 128))


def cut(array, low, high):
    def kernel(array, out):
        out[...] = array[low:high]

    return pl.pallas_call(
        kernel,
        out_shape=jax.ShapeDtypeStruct((high - low, *array.shape[1:]), BF16),
        in_specs=[VMEM],
        out_specs=VMEM,
        compiler_params=params(3),
        cost_estimate=cost(1 << 20),
    )(array)


def norm_rows(block, gain):
    residual = block.astype(F32)
    mean = jnp.mean(residual * residual, axis=1, keepdims=True)
    return (residual * lax.rsqrt(mean + EPS) * gain).astype(BF16)


def head_kernel(tokens, norm_gain, pool_gain, normed, gain_out):
    def norm(i, carry):
        rows = pl.multiple_of(i * 32, 32)
        normed[pl.ds(HALO + rows, 32)] = norm_rows(
            tokens[pl.ds(rows, 32)], norm_gain[0:1]
        )
        return carry

    lax.fori_loop(0, tokens.shape[0] // 32, norm, 0)
    old = lax.broadcasted_iota(jnp.int32, (512, 512), 0)
    new = lax.broadcasted_iota(jnp.int32, (512, 512), 1)
    source = new % 256 // 16 * 32 + new // 256 * 16 + new % 16
    gain_out[...] = jnp.dot(
        pool_gain[...],
        (old == source).astype(F32),
        precision=lax.Precision.HIGHEST,
        preferred_element_type=F32,
    )


def head(tokens, norm_gain, pool_gain):
    return pl.pallas_call(
        head_kernel,
        out_shape=(
            jax.ShapeDtypeStruct((HALO + tokens.shape[0], 2048), BF16),
            jax.ShapeDtypeStruct(pool_gain.shape, F32),
        ),
        in_specs=[VMEM] * 3,
        out_specs=(VMEM, VMEM),
        compiler_params=params(5),
        cost_estimate=cost(1 << 30),
        name="head",
    )(tokens, norm_gain, pool_gain)


def wholes():
    return (
        jax.ShapeDtypeStruct((2, 16, 16, 2048), BF16),
        jax.ShapeDtypeStruct((2, 2, 256, 2048), BF16),
    )


def placed(body, mib, inputs, state):
    rows = state[0].shape[0]
    count = len(inputs)

    def kernel(*refs):
        body(refs[:count], *refs[-4:])

    return pl.pallas_call(
        kernel,
        out_shape=(
            jax.ShapeDtypeStruct((rows, 2048), BF16),
            jax.ShapeDtypeStruct((2, rows, 256), F32),
            *wholes(),
        ),
        in_specs=[VMEM] * (count + len(state)),
        out_specs=(VMEM,) * 4,
        input_output_aliases={count + i: i for i in range(len(state))},
        compiler_params=params(mib),
        cost_estimate=cost(1 << 29),
    )(*inputs, *state)


def place_a(inputs, normed, total, whole_in, whole_down):
    mine, theirs = inputs
    c, s_mine, s_theirs = seconds()
    for slot, piece, core, second in ((0, mine, c, s_mine), (1, theirs, 1 - c, s_theirs)):
        s = along(second, 0)
        rows = slice(HALO, None)
        total[slot, rows] = part(normed, rows, piece, core, s)
        put_in(piece, core, s, whole_in)
    put_down((mine,), (theirs,), ((0, 0),), whole_down)


def place_b(inputs, normed, total, whole_in, whole_down):
    mine, theirs = inputs[:2], inputs[2:]
    c, s_mine, s_theirs = seconds()
    for slot, piece, core, second in (
        (0, mine[1], c, s_mine),
        (1, theirs[1], 1 - c, s_theirs),
    ):
        s = along(second, 1)
        rows = slice(HALO, None)
        total[slot, rows] += part(normed, rows, piece, core, s)
        put_in(piece, core, s, whole_in)
    put_down(mine, theirs, ((0, 1), (1, 0), (1, 1)), whole_down)


def place_d(inputs, normed, total, whole_in, whole_down):
    halo, norm_gain, *pieces = inputs
    mine, theirs = pieces[:3], pieces[3:]
    normed[:HALO] = norm_rows(halo[...], norm_gain[0:1])
    c, s_mine, s_theirs = seconds()
    for slot, of, core, second in ((0, mine, c, s_mine), (1, theirs, 1 - c, s_theirs)):
        rows = slice(0, HALO)
        total[slot, rows] = part(normed, rows, of[0], core, along(second, 0)) + part(
            normed, rows, of[1], core, along(second, 1)
        )
        s = along(second, 2)
        total[slot] += part(normed, slice(None), of[2], core, s)
        put_in(of[2], core, s, whole_in)
    put_down(mine, theirs, ((0, 2), (1, 2), (2, 0), (2, 1), (2, 2)), whole_down)


def place_c(inputs, normed, total, whole_in, whole_down):
    mine, theirs = (None, None, None, tuple(inputs[:2])), inputs[2:]
    c, s_mine, _ = seconds()
    s = along(s_mine, 3)
    total[0] += part(normed, slice(None), mine[3], c, s)
    put_in(mine[3], c, s, whole_in)
    put_down(mine, theirs, [(3, j) for j in range(3)], whole_down)


def mixer_kernel(tokens, halo, norm_gain, pool_gain, *refs):
    mine = (*refs[:3], tuple(refs[3:5]))
    theirs, left = (None, None, None, tuple(refs[5:7])), refs[7]
    out, total, whole_in, whole_down = refs[-10:-6]
    extended, pooled, middle, scaled, last, sems = refs[-6:]
    c, _, s_theirs = seconds()
    s = along(s_theirs, 3)
    put_in(theirs[3], 1 - c, s, whole_in)
    put_down(mine, theirs, [(k, 3) for k in range(4)], whole_down)
    rows = left.shape[0]
    extended[:PAD] = jnp.zeros((PAD, 512), F32)
    row = lax.broadcasted_iota(jnp.int32, (rows, 128), 0)
    lane = lax.broadcasted_iota(jnp.int32, (rows, 128), 1)
    position = lax.axis_index("sp") * 384 - HALO + row + 1
    position = jnp.maximum(position, 1).astype(F32)
    width = jnp.where(
        lane < 64, jnp.where(lane < 32, 2.0, 4.0), jnp.where(lane < 96, 8.0, 16.0)
    )
    share = 1.0 / jnp.minimum(position, width)

    def rounded(block):
        return block.astype(BF16).astype(F32)

    def pool(l):
        for j in range(4):
            lanes = slice(j * 128, (j + 1) * 128)
            own = extended[:, lanes]
            two = own + pltpu.roll(own, 1, 0)
            four = two + pltpu.roll(two, 2, 0)
            eight = four + pltpu.roll(four, 4, 0)
            sixteen = eight + pltpu.roll(eight, 8, 0)
            sums = jnp.where(
                lane < 64,
                jnp.where(lane < 32, two[PAD:], four[PAD:]),
                jnp.where(lane < 96, eight[PAD:], sixteen[PAD:]),
            )
            trailing = sums * share - own[PAD:]
            pooled[:, lanes] = (trailing * pool_gain[l : l + 1, lanes]).astype(BF16)

    extended[PAD:, pl.ds(pl.multiple_of(c * 256, 256), 256)] = rounded(total[0])
    extended[PAD:, pl.ds(pl.multiple_of((1 - c) * 256, 256), 256)] = rounded(
        total[1] + part(left, slice(None), theirs[3], 1 - c, s)
    )
    pool(0)
    squares = jnp.zeros((rows, 128), F32)
    for j in range(4):
        lanes = slice(j * 512, (j + 1) * 512)
        down = jnp.dot(
            pooled[...],
            whole_down[0, :, :, lanes].reshape(512, 512),
            preferred_element_type=F32,
        )
        before = jnp.concatenate([halo[:, lanes], tokens[:, lanes]], axis=0)
        middle[:, lanes] = (before.astype(F32) + down).astype(BF16)
        block = middle[:, lanes].astype(F32)
        scaled[:, lanes] = (block * norm_gain[1:2, lanes]).astype(BF16)
        block = block * block
        squares += (block[:, :128] + block[:, 128:256]) + (
            block[:, 256:384] + block[:, 384:]
        )
    mean = jnp.sum(squares, axis=1, keepdims=True) / 2048.0
    pool_in = lax.dot_general(
        scaled[...],
        whole_in[...].reshape(512, 2048),
        (((1,), (1,)), ((), ())),
        preferred_element_type=F32,
    )
    extended[PAD:] = rounded(pool_in * lax.rsqrt(mean + EPS))
    pool(1)
    copies = []
    for j in range(4):
        lanes = slice(j * 512, (j + 1) * 512)
        down = jnp.dot(
            pooled[HALO:],
            whole_down[1, :, :, lanes].reshape(512, 512),
            preferred_element_type=F32,
        )
        last[:, lanes] = (middle[HALO:, lanes].astype(F32) + down).astype(BF16)
        copies.append(
            pltpu.make_async_copy(last.at[:, lanes], out.at[:, lanes], sems.at[j])
        )
        copies[-1].start()
    for copy in copies:
        copy.wait()


def mixer(tokens, halo, norm_gain, pool_gain, pieces, state):
    rows = state[0].shape[0]
    at = 5 + len(pieces)
    return pl.pallas_call(
        mixer_kernel,
        out_shape=(
            jax.ShapeDtypeStruct(tokens.shape, tokens.dtype),
            jax.ShapeDtypeStruct((2, rows, 256), F32),
            *wholes(),
        ),
        in_specs=[VMEM] * (at + 3),
        out_specs=(pl.BlockSpec(memory_space=pl.ANY),) + (VMEM,) * 3,
        input_output_aliases={at: 1, at + 1: 2, at + 2: 3},
        scratch_shapes=[
            pltpu.VMEM((PAD + rows, 512), F32),
            pltpu.VMEM((rows, 512), BF16),
            pltpu.VMEM((rows, 2048), BF16),
            pltpu.VMEM((rows, 2048), BF16),
            pltpu.VMEM(tokens.shape, BF16),
            pltpu.SemaphoreType.DMA((4,)),
        ],
        compiler_params=params(16),
        cost_estimate=cost(4 << 30),
        name="mixer",
    )(tokens, halo, norm_gain, pool_gain, *pieces, *state)[0]


def mixed(tokens, norm_gain, in_weight, down_weight, pool_gain):
    rows = tokens.shape[1]
    end = cut(tokens[0], rows - HALO, rows)
    halo = lax.ppermute(end, AXES, [(i, i + 32) for i in range(480)])
    normed, pool_gain = head(tokens[0], norm_gain, pool_gain)
    column = shared(packed(in_weight, down_weight), lambda y, x, z, c: (y, x, c))
    line = shared(
        jnp.broadcast_to(column[None], (4, 16, 64, 128)),
        lambda y, x, z, c: (y, z, c) if c == 0 else (x, z, c),
    )
    up = send(line, second_hop(1))
    down = send(line, second_hop(-1))
    up_on = send(cut(up, 0, 2), second_hop(1))
    down_on = send(cut(down, 2, 4), second_hop(-1))
    mine = [line, up, down, up_on, down_on]
    theirs = [send(piece, other_core) for piece in mine]
    state = placed(place_a, 10, mine[:1] + theirs[:1], (normed,))
    inputs = [halo, norm_gain, *mine[:3], *theirs[:3]]
    state = placed(place_b, 10, mine[:2] + theirs[:2], state)
    state = placed(place_d, 10, inputs, state)
    state = placed(place_c, 10, mine[3:] + theirs[:3], state)
    pieces = mine + theirs[3:]
    return mixer(tokens[0], halo, norm_gain, pool_gain, pieces, state)[None]


def solution(mesh):
    in_specs = (P("tp", "sp", None), P(), P(None, "sp", "tp"), P(None, "sp", "tp"), P())
    out_specs = P("tp", "sp", None)
    return jax.shard_map(
        mixed, mesh=mesh, in_specs=in_specs, out_specs=out_specs, check_vma=False
    )
```

```python
import jax
import jax.numpy as jnp
from jax import lax
from jax.experimental import pallas as pl
from jax.experimental.pallas import tpu as pltpu
from jax.sharding import PartitionSpec as P

EPS = 1e-06
HALO = 32
PAD = 16
AXES = ("sp", "tp")
PIECES = (0, -1, 1, 2)
VMEM = pl.BlockSpec(memory_space=pltpu.VMEM)
BF16, F32 = jnp.bfloat16, jnp.float32


def number(y, x, z, c):
    return (((y % 4) * 4 + x % 4) * 16 + z % 16) * 2 + c


def places():
    for i in range(512):
        yield i, (i // 128, i // 32 % 4, i // 2 % 16, i % 2)


def send(block, target):
    route = [(i, number(*target(*place))) for i, place in places()]
    return lax.ppermute(block, AXES, route)


def shared(copies, key):
    groups = {}
    for i, place in places():
        groups.setdefault(key(*place), []).append(i)
    return lax.all_to_all(
        copies, AXES, 0, 0, axis_index_groups=list(groups.values()), tiled=True
    )


def second_hop(d):
    return lambda y, x, z, c: (y + d, x, z, c) if c == 0 else (y, x + d, z, c)


def other_core(y, x, z, c):
    return y, x, z, 1 - c


def seconds():
    sp, c = lax.axis_index("sp"), lax.axis_index("tp") % 2
    y, x = sp // 4, sp % 4
    return c, jnp.where(c == 0, y, x), jnp.where(c == 0, x, y)


def lanes_of(core, s, f):
    at = jnp.where(core == 0, s * 4 + f, f * 4 + s)
    return pl.ds(pl.multiple_of(at * 128, 128), 128)


def along(second, k):
    return (second + PIECES[k] + 4) % 4


def of_first(piece, f):
    return piece[f // 2].at[f % 2] if isinstance(piece, tuple) else piece.at[f]


def down_tile(piece, f, z):
    if not isinstance(piece, tuple):
        return piece[f, z, 32:64]
    low, high = (half[f % 2, z, 32:64] for half in piece)
    return jnp.where(f < 2, low, high)


def part(left, rows, piece, core, s):
    lhs = jnp.concatenate([left[rows, lanes_of(core, s, f)] for f in range(4)], axis=1)
    rhs = jnp.concatenate(
        [of_first(piece, f)[:, 0:16].reshape(256, 128) for f in range(4)], axis=1
    )
    return lax.dot_general(
        lhs, rhs, (((1,), (1,)), ((), ())), preferred_element_type=F32
    )


def put_in(piece, core, s, whole_in):
    for f in range(4):
        whole_in[core, :, :, lanes_of(core, s, f)] = of_first(piece, f)[:, 16:32]


def put_down(mine, theirs, pairs, whole_down):
    c, s_mine, s_theirs = seconds()
    left = (lax.broadcasted_iota(jnp.int32, (32, 128), 1) < 64) ^ (c == 1)
    for k, j in pairs:
        a, b = along(s_mine, k), along(s_theirs, j)
        at = jnp.where(c == 0, a * 4 + b, b * 4 + a)
        rows = pl.ds(pl.multiple_of(at * 16, 16), 16)
        for z in range(16):
            m = down_tile(mine[k], b, z)
            t = down_tile(theirs[j], a, z)
            lanes = slice(z * 128, (z + 1) * 128)
            first = jnp.where(left, m, t)
            last = jnp.where(left, t, m)
            last = jnp.concatenate([last[:, 64:], last[:, :64]], axis=1)
            for l, tile in enumerate((first, last)):
                whole_down[l, 0, rows, lanes] = tile[:16]
                whole_down[l, 1, rows, lanes] = tile[16:]


def params(mib):
    return pltpu.CompilerParams(vmem_limit_bytes=mib << 20)


def cost(flops):
    return pl.CostEstimate(flops=flops, bytes_accessed=1 << 20, transcendentals=0)


def pack_kernel(turned, down, out):
    c = lax.axis_index("tp") % 2
    first = jnp.where(c == 0, down[0], down[1])
    last = jnp.where(c == 0, down[1], down[0])
    folded = jnp.concatenate([first, last], axis=1)
    for z in range(16):
        out[z, 0:16] = turned[0]
        out[z, 16:32] = turned[1]
        out[z, 32:64] = folded


def packed(in_weight, down_weight):
    return pl.pallas_call(
        pack_kernel,
        out_shape=jax.ShapeDtypeStruct((16, 64, 128), BF16),
        in_specs=[VMEM] * 2,
        out_specs=VMEM,
        compiler_params=params(2),
        cost_estimate=cost(1 << 20),
        name="pack",
    )(jnp.swapaxes(in_weight, 1, 2), down_weight)


def cut(array, low, high):
    def kernel(array, out):
        out[...] = array[low:high]

    return pl.pallas_call(
        kernel,
        out_shape=jax.ShapeDtypeStruct((high - low, *array.shape[1:]), BF16),
        in_specs=[VMEM],
        out_specs=VMEM,
        compiler_params=params(3),
        cost_estimate=cost(1 << 20),
    )(array)


def norm_rows(block, gain):
    residual = block.astype(F32)
    mean = jnp.mean(residual * residual, axis=1, keepdims=True)
    return (residual * lax.rsqrt(mean + EPS) * gain).astype(BF16)


def head_kernel(tokens, norm_gain, pool_gain, normed, gain_out):
    def norm(i, carry):
        rows = pl.multiple_of(i * 32, 32)
        normed[pl.ds(HALO + rows, 32)] = norm_rows(
            tokens[pl.ds(rows, 32)], norm_gain[0:1]
        )
        return carry

    lax.fori_loop(0, tokens.shape[0] // 32, norm, 0)
    old = lax.broadcasted_iota(jnp.int32, (512, 512), 0)
    new = lax.broadcasted_iota(jnp.int32, (512, 512), 1)
    source = new % 256 // 16 * 32 + new // 256 * 16 + new % 16
    gain_out[...] = jnp.dot(
        pool_gain[...],
        (old == source).astype(F32),
        precision=lax.Precision.HIGHEST,
        preferred_element_type=F32,
    )


def head(tokens, norm_gain, pool_gain):
    return pl.pallas_call(
        head_kernel,
        out_shape=(
            jax.ShapeDtypeStruct((HALO + tokens.shape[0], 2048), BF16),
            jax.ShapeDtypeStruct(pool_gain.shape, F32),
        ),
        in_specs=[VMEM] * 3,
        out_specs=(VMEM, VMEM),
        compiler_params=params(5),
        cost_estimate=cost(1 << 30),
        name="head",
    )(tokens, norm_gain, pool_gain)


def wholes():
    return (
        jax.ShapeDtypeStruct((2, 16, 16, 2048), BF16),
        jax.ShapeDtypeStruct((2, 2, 256, 2048), BF16),
    )


def placed(body, mib, inputs, state):
    rows = state[0].shape[0]
    count = len(inputs)

    def kernel(*refs):
        body(refs[:count], *refs[-4:])

    return pl.pallas_call(
        kernel,
        out_shape=(
            jax.ShapeDtypeStruct((rows, 2048), BF16),
            jax.ShapeDtypeStruct((2, rows, 256), F32),
            *wholes(),
        ),
        in_specs=[VMEM] * (count + len(state)),
        out_specs=(VMEM,) * 4,
        input_output_aliases={count + i: i for i in range(len(state))},
        compiler_params=params(mib),
        cost_estimate=cost(1 << 29),
    )(*inputs, *state)


def place_a(inputs, normed, total, whole_in, whole_down):
    mine, theirs = inputs
    c, s_mine, s_theirs = seconds()
    for slot, piece, core, second in ((0, mine, c, s_mine), (1, theirs, 1 - c, s_theirs)):
        s = along(second, 0)
        rows = slice(HALO, None)
        total[slot, rows] = part(normed, rows, piece, core, s)
        put_in(piece, core, s, whole_in)
    put_down((mine,), (theirs,), ((0, 0),), whole_down)


def place_b(inputs, normed, total, whole_in, whole_down):
    mine, theirs = inputs[:2], inputs[2:]
    c, s_mine, s_theirs = seconds()
    for slot, piece, core, second in (
        (0, mine[1], c, s_mine),
        (1, theirs[1], 1 - c, s_theirs),
    ):
        s = along(second, 1)
        rows = slice(HALO, None)
        total[slot, rows] += part(normed, rows, piece, core, s)
        put_in(piece, core, s, whole_in)
    put_down(mine, theirs, ((0, 1), (1, 0), (1, 1)), whole_down)


def place_d(inputs, normed, total, whole_in, whole_down):
    halo, norm_gain, *pieces = inputs
    mine, theirs = pieces[:3], pieces[3:]
    normed[:HALO] = norm_rows(halo[...], norm_gain[0:1])
    c, s_mine, s_theirs = seconds()
    for slot, of, core, second in ((0, mine, c, s_mine), (1, theirs, 1 - c, s_theirs)):
        rows = slice(0, HALO)
        total[slot, rows] = part(normed, rows, of[0], core, along(second, 0)) + part(
            normed, rows, of[1], core, along(second, 1)
        )
        s = along(second, 2)
        total[slot] += part(normed, slice(None), of[2], core, s)
        put_in(of[2], core, s, whole_in)
    put_down(mine, theirs, ((0, 2), (1, 2), (2, 0), (2, 1), (2, 2)), whole_down)


def place_c(inputs, normed, total, whole_in, whole_down):
    mine, theirs = (None, None, None, tuple(inputs[:2])), inputs[2:]
    c, s_mine, _ = seconds()
    s = along(s_mine, 3)
    total[0] += part(normed, slice(None), mine[3], c, s)
    put_in(mine[3], c, s, whole_in)
    put_down(mine, theirs, [(3, j) for j in range(3)], whole_down)


def mixer_kernel(tokens, halo, norm_gain, pool_gain, *refs):
    mine = (*refs[:3], tuple(refs[3:5]))
    theirs, left = (None, None, None, tuple(refs[5:7])), refs[7]
    out, total, whole_in, whole_down = refs[-10:-6]
    extended, pooled, middle, scaled, last, sems = refs[-6:]
    c, _, s_theirs = seconds()
    s = along(s_theirs, 3)
    put_in(theirs[3], 1 - c, s, whole_in)
    put_down(mine, theirs, [(k, 3) for k in range(4)], whole_down)
    rows = left.shape[0]
    extended[:PAD] = jnp.zeros((PAD, 512), F32)
    row = lax.broadcasted_iota(jnp.int32, (rows, 128), 0)
    lane = lax.broadcasted_iota(jnp.int32, (rows, 128), 1)
    position = lax.axis_index("sp") * 384 - HALO + row + 1
    position = jnp.maximum(position, 1).astype(F32)
    width = jnp.where(
        lane < 64, jnp.where(lane < 32, 2.0, 4.0), jnp.where(lane < 96, 8.0, 16.0)
    )
    share = 1.0 / jnp.minimum(position, width)

    def rounded(block):
        return block.astype(BF16).astype(F32)

    def pool(l):
        for j in range(4):
            lanes = slice(j * 128, (j + 1) * 128)
            own = extended[:, lanes]
            two = own + pltpu.roll(own, 1, 0)
            four = two + pltpu.roll(two, 2, 0)
            eight = four + pltpu.roll(four, 4, 0)
            sixteen = eight + pltpu.roll(eight, 8, 0)
            sums = jnp.where(
                lane < 64,
                jnp.where(lane < 32, two[PAD:], four[PAD:]),
                jnp.where(lane < 96, eight[PAD:], sixteen[PAD:]),
            )
            trailing = sums * share - own[PAD:]
            pooled[:, lanes] = (trailing * pool_gain[l : l + 1, lanes]).astype(BF16)

    extended[PAD:, pl.ds(pl.multiple_of(c * 256, 256), 256)] = rounded(total[0])
    extended[PAD:, pl.ds(pl.multiple_of((1 - c) * 256, 256), 256)] = rounded(
        total[1] + part(left, slice(None), theirs[3], 1 - c, s)
    )
    pool(0)
    squares = jnp.zeros((rows, 128), F32)
    for j in range(4):
        lanes = slice(j * 512, (j + 1) * 512)
        down = jnp.dot(
            pooled[...],
            whole_down[0, :, :, lanes].reshape(512, 512),
            preferred_element_type=F32,
        )
        before = jnp.concatenate([halo[:, lanes], tokens[:, lanes]], axis=0)
        middle[:, lanes] = (before.astype(F32) + down).astype(BF16)
        block = middle[:, lanes].astype(F32)
        scaled[:, lanes] = (block * norm_gain[1:2, lanes]).astype(BF16)
        block = block * block
        squares += (block[:, :128] + block[:, 128:256]) + (
            block[:, 256:384] + block[:, 384:]
        )
    mean = jnp.sum(squares, axis=1, keepdims=True) / 2048.0
    pool_in = lax.dot_general(
        scaled[...],
        whole_in[...].reshape(512, 2048),
        (((1,), (1,)), ((), ())),
        preferred_element_type=F32,
    )
    extended[PAD:] = rounded(pool_in * lax.rsqrt(mean + EPS))
    pool(1)
    copies = []
    for j in range(4):
        lanes = slice(j * 512, (j + 1) * 512)
        down = jnp.dot(
            pooled[HALO:],
            whole_down[1, :, :, lanes].reshape(512, 512),
            preferred_element_type=F32,
        )
        last[:, lanes] = (middle[HALO:, lanes].astype(F32) + down).astype(BF16)
        copies.append(
            pltpu.make_async_copy(last.at[:, lanes], out.at[:, lanes], sems.at[j])
        )
        copies[-1].start()
    for copy in copies:
        copy.wait()


def mixer(tokens, halo, norm_gain, pool_gain, pieces, state):
    rows = state[0].shape[0]
    at = 5 + len(pieces)
    return pl.pallas_call(
        mixer_kernel,
        out_shape=(
            jax.ShapeDtypeStruct(tokens.shape, tokens.dtype),
            jax.ShapeDtypeStruct((2, rows, 256), F32),
            *wholes(),
        ),
        in_specs=[VMEM] * (at + 3),
        out_specs=(pl.BlockSpec(memory_space=pl.ANY),) + (VMEM,) * 3,
        input_output_aliases={at: 1, at + 1: 2, at + 2: 3},
        scratch_shapes=[
            pltpu.VMEM((PAD + rows, 512), F32),
            pltpu.VMEM((rows, 512), BF16),
            pltpu.VMEM((rows, 2048), BF16),
            pltpu.VMEM((rows, 2048), BF16),
            pltpu.VMEM(tokens.shape, BF16),
            pltpu.SemaphoreType.DMA((4,)),
        ],
        compiler_params=params(16),
        cost_estimate=cost(4 << 30),
        name="mixer",
    )(tokens, halo, norm_gain, pool_gain, *pieces, *state)[0]


def mixed(tokens, norm_gain, in_weight, down_weight, pool_gain):
    rows = tokens.shape[1]
    end = cut(tokens[0], rows - HALO, rows)
    halo = lax.ppermute(end, AXES, [(i, i + 32) for i in range(480)])
    normed, pool_gain = head(tokens[0], norm_gain, pool_gain)
    column = shared(packed(in_weight, down_weight), lambda y, x, z, c: (y, x, c))
    line = shared(
        jnp.broadcast_to(column[None], (4, 16, 64, 128)),
        lambda y, x, z, c: (y, z, c) if c == 0 else (x, z, c),
    )
    up = send(line, second_hop(1))
    down = send(line, second_hop(-1))
    up_on = send(cut(up, 0, 2), second_hop(1))
    down_on = send(cut(down, 2, 4), second_hop(-1))
    mine = [line, up, down, up_on, down_on]
    theirs = [send(piece, other_core) for piece in mine]
    state = placed(place_a, 10, mine[:1] + theirs[:1], (normed,))
    inputs = [halo, norm_gain, *mine[:3], *theirs[:3]]
    state = placed(place_b, 10, mine[:2] + theirs[:2], state)
    state = placed(place_d, 10, inputs, state)
    state = placed(place_c, 10, mine[3:] + theirs[:3], state)
    pieces = mine + theirs[3:]
    return mixer(tokens[0], halo, norm_gain, pool_gain, pieces, state)[None]


def solution(mesh):
    in_specs = (P("tp", "sp", None), P(), P(None, "sp", "tp"), P(None, "sp", "tp"), P())
    out_specs = P("tp", "sp", None)
    return jax.shard_map(
        mixed, mesh=mesh, in_specs=in_specs, out_specs=out_specs, check_vma=False
    )
```
